32 devices in a mesh: ep: 16 (over z, y, x), tp: 2 (over core).
Axes of the slice: x: 2, y: 2, z: 4, core: 2. Of those that a mesh axis runs over, the one named last changes fastest.
Arguments:
- tokens: bfloat16 [4096, 2048], P(('ep', 'tp')), may hold values from -6 to 6
- norm_gain: float32 [2048], replicated, may hold values from 0.25 to 4
- routes: int32 [4096, 2], P(('ep', 'tp')), may hold values from 0 to 15, all different within a row; in each aligned block of 128 rows (0 to 127, 128 to 255, ...) at most 22 rows name the same one
- route_weights: float32 [4096, 2], P(('ep', 'tp')), may hold values from 0.1 to 1
- w_gate: bfloat16 [16, 2048, 1024], P('ep', None, 'tp'), may hold values from -0.125 to 0.125
- w_up: bfloat16 [16, 2048, 1024], P('ep', None, 'tp'), may hold values from -0.125 to 0.125
- w_down: bfloat16 [16, 1024, 2048], P('ep', 'tp'), may hold values from -0.1875 to 0.1875
- dense_in: bfloat16 [2048, 256], P('ep'), may hold values from -0.125 to 0.125
- dense_out: bfloat16 [2048, 256], P('ep'), may hold values from -0.375 to 0.375
- dense_gate: float32 [2048], replicated, may hold values from -6 to 6
Outputs:
- mixed: bfloat16 [4096, 2048], P(('ep', 'tp'))
The draws below stay inside these ranges and needn't reach their ends.
Inputs may be any that keep to these rules, and one draw needn't show every extreme that they name: `routes`: each row names 2 different experts. Among the 128 rows of one device no expert is named more than 22 times; every draw has a device and an expert with exactly 22.
All inputs are finite; a program needn't handle non-finite values.
Results may differ from the reference program's by a relative error of at most 0.0074.
Values may be sent and summed in bfloat16 or wider, within the bound.
No kernel may reach another device: no remote copies, remote signals or barrier semaphores. Data moves between devices by JAX's collectives and lax.ppermute only.
A program may use at most 128 MiB of HBM per device.

```python
import math
import jax
import jax.numpy as jnp
import numpy as np
from jax import lax

D = 2048
FF = 1024
DH = 256
TOP_K = 2
TOK_DEV = 128
EXPERTS = 16
TOKENS = 4096
CAP = 22
N_TP = 2


def draw_norm_gain(key, part):
    return 1.0 + 0.18 * jnp.clip(jax.random.normal(key, (D,), jnp.float32), -4.0, 4.0)


def shard_levels(key, shape, pieces, low, largest):
    factor_of = 1.0
    for axis_at, blocks in pieces:
        steps = jax.random.uniform(jax.random.fold_in(jax.random.fold_in(key, 6), axis_at), (blocks,), jnp.float32, low / len(pieces), largest / len(pieces))
        factor_of = factor_of * jnp.repeat(jnp.exp(steps), shape[axis_at] // blocks).reshape((-1,) + (1,) * (len(shape) - 1 - axis_at))
    return factor_of


def assign_block(own_key, own, number, rows, amount, top, bound, slope):
    order = jax.random.permutation(own_key, amount)
    packed, common = portions_of(amount, rows * top, bound, slope, True), portions_of(amount, rows * top, bound, slope, False)
    places = jnp.arange(amount)

    def named(lengths, turn):
        used = int((lengths > 0).sum())
        fixed = max(1, used // 4)
        passed = fixed + (places - fixed + turn * (used - fixed)) % max(1, amount - fixed)
        return jnp.zeros((amount,), jnp.int32).at[order[jnp.where(places < fixed, places, passed)]].set(jnp.asarray(lengths, jnp.int32))

    lengths = jnp.where(number % 4 == 0, named(packed, number // 4), named(common, number - number // 4 - 1))
    mixed = jax.random.permutation(jax.random.fold_in(own, 3), amount)
    donor, sink = mixed[0:amount // 2 * 2:2], mixed[1:amount // 2 * 2:2]
    margin = jnp.minimum(lengths[donor] - 1, bound - lengths[sink]) // 2
    margin = jnp.where((donor == order[0]) | (sink == order[0]) | (lengths[sink] == 0), 0, jnp.maximum(margin, 0))
    passed = jax.random.randint(jax.random.fold_in(own, 4), (amount // 2,), 0, 1 << 20) % (margin + 1)
    lengths = lengths.at[donor].add(-passed).at[sink].add(passed)
    items = jnp.searchsorted(jnp.cumsum(lengths), jnp.arange(rows * top), side="right").astype(jnp.int32)
    table = items.reshape(top, rows).T
    table = table[jax.random.permutation(jax.random.fold_in(own, 1), rows)]
    turn = jax.random.randint(jax.random.fold_in(own, 2), (rows, 1), 0, top)
    return jnp.take_along_axis(table, (jnp.arange(top)[None, :] + turn) % top, axis=1)


def portions_of(amount, total, reach, skew, full):
    loads = [(1 << 20) // math.isqrt(standing ** skew) + 1 for standing in range(1, amount + 1)]
    largest = reach if full else min(reach, max(-(-total // amount), total * loads[0] // sum(loads)))
    least = 1 if total - largest >= amount - 1 else 0
    given, spare = [largest] + [least] * (amount - 1), total - largest - least * (amount - 1)
    while spare > 0:
        free = [i for i in range(1, amount) if given[i] < largest] or [i for i in range(1, amount) if given[i] < reach]
        mass, left = sum([loads[i] for i in free]), spare
        for i in free:
            addition = min(reach - given[i], max(1, left * loads[i] // mass), spare)
            given[i] = given[i] + addition
            spare = spare - addition
    return np.array(given)


def noise(rng, dims, width, reach, split=(), kind=jnp.bfloat16):
    array = jax.random.normal(rng, dims, jnp.float32) * width
    if len(split) > 0:
        array = shard_levels(rng, dims, split, -0.22, 0.18) * array
    return jnp.clip(array, min=-reach, max=reach).astype(kind)


def setup_inputs(seed: int = 0) -> dict:
    key_of = jax.random.split(jax.random.key(seed), 11)
    tokens = noise(key_of[0], (TOKENS, D), 1.0, 6.0, ((0, 32),))
    norm_gain = draw_norm_gain(jax.random.fold_in(key_of[10], 71), 0)
    routes_keys = jax.random.split(jax.random.fold_in(key_of[2], 1), TOKENS // TOK_DEV)
    routes_turns = jax.random.permutation(jax.random.fold_in(key_of[2], 3), TOKENS // TOK_DEV)
    routes = jax.vmap(lambda own, number: assign_block(jax.random.fold_in(key_of[2], 2), own, number, TOK_DEV, EXPERTS, TOP_K, CAP, 2))(routes_keys, routes_turns).reshape((TOKENS, TOP_K))
    route_weights = jnp.clip(0.1 + 0.9 * jax.random.uniform(key_of[3], (TOKENS, TOP_K), jnp.float32) ** shard_levels(key_of[3], (TOKENS, TOP_K), ((0, 32),), -0.2, 0.2), 0.1, 1.0)
    w_gate = noise(key_of[4], (EXPERTS, D, FF), D ** -0.5, 0.125, ((0, 16), (2, 2)))
    w_up = noise(key_of[5], (EXPERTS, D, FF), D ** -0.5, 0.125, ((0, 16), (2, 2)))
    w_down = noise(key_of[6], (EXPERTS, FF, D), FF ** -0.5, 0.1875, ((0, 16), (1, 2)))
    dense_in = noise(key_of[7], (D, DH), D ** -0.5, 0.125, ((0, 16),))
    dense_out = noise(key_of[8], (D, DH), DH ** -0.5, 0.375, ((0, 16),))
    dense_gate = noise(key_of[9], (D,), 1.5, 6.0, (), jnp.float32)
    return dict(tokens=tokens, norm_gain=norm_gain, routes=routes, route_weights=route_weights, w_gate=w_gate, w_up=w_up, w_down=w_down, dense_in=dense_in, dense_out=dense_out, dense_gate=dense_gate)


CLAMP_LIMIT = 7.0
SLOPE_ALPHA = 1.702
NORM_EPS = 1e-06

def rms_normed(tokens, norm_gain):
    widened = tokens.astype(jnp.float32)
    inv_scale = lax.rsqrt(lax.optimization_barrier(jnp.mean(widened * widened, axis=1, keepdims=True)) + NORM_EPS)
    return (widened * inv_scale * norm_gain).astype(jnp.bfloat16)

def clamped_unit(gate_pre, up_pre):
    gate_clip = jnp.minimum(gate_pre, CLAMP_LIMIT)
    up_clip = jnp.clip(up_pre, -CLAMP_LIMIT, CLAMP_LIMIT)
    return ((up_clip + 1.0) * gate_clip * jax.nn.sigmoid(SLOPE_ALPHA * gate_clip)).astype(jnp.bfloat16)

def reference(tokens, norm_gain, routes, route_weights, w_gate, w_up, w_down, dense_in, dense_out, dense_gate):
    normed = rms_normed(tokens, norm_gain)
    sources = TOKENS // TOK_DEV
    entries = TOK_DEV * TOP_K
    block_routes = routes.reshape(sources, entries)
    onehot = (block_routes[:, :, None] == jnp.arange(EXPERTS, dtype=jnp.int32)[None, None, :]).astype(jnp.int32)
    slot_index = lax.optimization_barrier(jnp.sum((jnp.cumsum(onehot, axis=1) - onehot) * onehot, axis=2))
    source_ids = jnp.arange(sources, dtype=jnp.int32)[:, None]
    position = (block_routes * (sources * CAP) + source_ids * CAP + slot_index).reshape(-1).astype(jnp.int32)
    entry_ids = jnp.arange(TOKENS * TOP_K, dtype=jnp.int32)
    slot_table = jnp.full((EXPERTS * sources * CAP,), -1, jnp.int32).at[position].set(entry_ids)
    slot_table = slot_table.reshape(EXPERTS, sources * CAP)
    half_width = FF // N_TP

    def one_expert(expert_args):
        entry_index, gate_w, up_w, down_w = expert_args
        is_valid = entry_index >= 0
        token_of = jnp.where(is_valid, entry_index, 0) // TOP_K
        gathered_rows = jnp.where(is_valid[:, None], normed[token_of], jnp.zeros((), jnp.bfloat16))
        gate_pre = jnp.dot(gathered_rows, gate_w, preferred_element_type=jnp.float32)
        up_pre = jnp.dot(gathered_rows, up_w, preferred_element_type=jnp.float32)
        hidden = clamped_unit(gate_pre, up_pre)
        summed = jnp.zeros((gathered_rows.shape[0], D), jnp.float32)
        for half_index in range(N_TP):
            low = half_index * half_width
            partial_value = jnp.dot(hidden[:, low:low + half_width], down_w[low:low + half_width], preferred_element_type=jnp.float32).astype(jnp.bfloat16)
            summed = summed + lax.optimization_barrier(partial_value).astype(jnp.float32)
        return summed.astype(jnp.bfloat16)
    results = lax.map(one_expert, (slot_table, w_gate, w_up, w_down))
    flat_results = results.reshape(EXPERTS * sources * CAP, D)
    picked = flat_results[position].astype(jnp.float32).reshape(TOKENS, TOP_K, D)
    weighted = lax.optimization_barrier(jnp.sum(picked * route_weights[:, :, None], axis=1))
    dense_hidden = jax.nn.silu(jnp.dot(normed, dense_in, preferred_element_type=jnp.float32)).astype(jnp.bfloat16)
    branch = lax.dot_general(dense_hidden, dense_out, (((1,), (1,)), ((), ())), preferred_element_type=jnp.float32)
    return (weighted + jax.nn.sigmoid(dense_gate) * branch).astype(jnp.bfloat16)
```

```python
import math

import jax
import jax.numpy as jnp
from jax import lax
from jax.experimental import pallas as pl
from jax.experimental.pallas import tpu as pltpu
from jax.sharding import PartitionSpec as P

CLAMP_LIMIT = 7.0
SLOPE_ALPHA = 1.702
NORM_EPS = 1e-06
VMEM = pl.BlockSpec(memory_space=pltpu.VMEM)
SMEM = pl.BlockSpec(memory_space=pltpu.SMEM)
LIMIT = 40 * 1024 * 1024


def capacity_of(tok_rows, top_count, experts):
    return (4 * tok_rows * top_count + 3 * experts - 1) // (3 * experts)


def rms_normed(tokens, norm_gain):
    widened = tokens.astype(jnp.float32)
    inv_scale = lax.rsqrt(jnp.mean(widened * widened, axis=1, keepdims=True) + NORM_EPS)
    return (widened * inv_scale * norm_gain).astype(jnp.bfloat16)


def clamped_unit(gate_pre, up_pre):
    gate_clip = jnp.minimum(gate_pre, CLAMP_LIMIT)
    up_clip = jnp.clip(up_pre, -CLAMP_LIMIT, CLAMP_LIMIT)
    return ((up_clip + 1.0) * gate_clip * jax.nn.sigmoid(SLOPE_ALPHA * gate_clip)).astype(
        jnp.bfloat16
    )


def slot_ranks(route_cols, me, offsets):
    tok_rows = route_cols.shape[1]
    count = len(offsets)
    row = lax.broadcasted_iota(jnp.int32, (count, 1), 0)
    expert = jnp.bitwise_xor(row, me)
    chosen = route_cols[0:1, :] == expert
    for choice in range(1, route_cols.shape[0]):
        chosen = chosen | (route_cols[choice : choice + 1, :] == expert)
    earlier = (
        lax.broadcasted_iota(jnp.int32, (tok_rows, tok_rows), 0)
        < lax.broadcasted_iota(jnp.int32, (tok_rows, tok_rows), 1)
    )
    counted = jnp.dot(
        jnp.where(chosen, 1.0, 0.0).astype(jnp.bfloat16),
        jnp.where(earlier, 1.0, 0.0).astype(jnp.bfloat16),
        preferred_element_type=jnp.float32,
    )
    return jnp.where(chosen, counted, -1.0)


def pack_kernel(blocks, rows, me_ref, tok_ref, gain_ref, route_ref, norm_ref, *send_refs):
    normed = rms_normed(tok_ref[...], gain_ref[...])
    norm_ref[...] = normed
    ranks = slot_ranks(route_ref[...], me_ref[0], range(blocks))
    slot = lax.broadcasted_iota(jnp.int32, (rows, 1), 0).astype(jnp.float32)
    select = jnp.concatenate(
        [jnp.where(ranks[k : k + 1, :] == slot, 1.0, 0.0) for k in range(blocks)], axis=0
    ).astype(jnp.bfloat16)
    packed = jnp.dot(select, normed, preferred_element_type=jnp.float32).astype(jnp.bfloat16)
    for k in range(blocks):
        send_refs[k][...] = packed[k * rows : (k + 1) * rows, :]


def expert_kernel(count, rows, *refs):
    row_refs, refs = refs[:count], refs[count:]
    (gate0, up0, down0, gate1, up1, down1), out_refs = refs[:6], refs[6:]
    flat = jnp.concatenate([r[...] for r in row_refs], axis=0)
    total = None
    for gate_ref, up_ref, down_ref in ((gate0, up0, down0), (gate1, up1, down1)):
        hidden = clamped_unit(
            jnp.dot(flat, gate_ref[...], preferred_element_type=jnp.float32),
            jnp.dot(flat, up_ref[...], preferred_element_type=jnp.float32),
        )
        part = jnp.dot(hidden, down_ref[...], preferred_element_type=jnp.float32)
        part = part.astype(jnp.bfloat16).astype(jnp.float32)
        total = part if total is None else total + part
    total = total.astype(jnp.bfloat16)
    for k in range(count):
        out_refs[k][...] = total[k * rows : (k + 1) * rows, :]


def weigh_kernel(blocks, rows, me_ref, route_ref, weight_ref, high_ref, low_ref):
    route_cols = route_ref[...]
    weights = weight_ref[...]
    ranks = slot_ranks(route_cols, me_ref[0], range(blocks))
    expert = jnp.bitwise_xor(lax.broadcasted_iota(jnp.int32, (blocks, 1), 0), me_ref[0])
    scale = jnp.zeros(ranks.shape, jnp.float32)
    for choice in range(route_cols.shape[0]):
        hit = route_cols[choice : choice + 1, :] == expert
        scale = scale + jnp.where(hit, weights[choice : choice + 1, :], 0.0)
    slot = lax.broadcasted_iota(jnp.int32, (rows, 1), 0).astype(jnp.float32)
    table = jnp.concatenate(
        [
            jnp.where(ranks[k : k + 1, :] == slot, scale[k : k + 1, :], 0.0)
            for k in range(blocks)
        ],
        axis=0,
    ).T
    high = table.astype(jnp.bfloat16)
    high_ref[...] = high
    low_ref[...] = (table - high.astype(jnp.float32)).astype(jnp.bfloat16)


def hidden_kernel(order, me_ref, core_ref, norm_ref, mine_ref, other_ref, out_ref):
    shard = mine_ref.shape[0] // len(order)

    def run(source):
        total = None
        for place, offset in enumerate(order):
            at = pl.multiple_of(jnp.bitwise_xor(me_ref[0], offset) * shard, shard)
            part = jnp.dot(
                norm_ref[:, pl.ds(at, shard)],
                source[place * shard : (place + 1) * shard, :],
                preferred_element_type=jnp.float32,
            )
            total = part if total is None else total + part
        out_ref[...] = (total / (1.0 + jnp.exp(-total))).astype(jnp.bfloat16)

    @pl.when(core_ref[0] == 0)
    def _():
        run(mine_ref)

    @pl.when(core_ref[0] != 0)
    def _():
        run(other_ref)


def combine_kernel(blocks, rows, order, me_ref, core_ref, high_ref, low_ref, hid_ref, mine_ref,
                   other_ref, dgate_ref, *refs):
    row_refs, out_ref, branch_ref = refs[:blocks], refs[blocks], refs[blocks + 1]
    shard = mine_ref.shape[0] // len(order)

    def run(source):
        for place, offset in enumerate(order):
            at = pl.multiple_of(jnp.bitwise_xor(me_ref[0], offset) * shard, shard)
            branch_ref[:, pl.ds(at, shard)] = lax.dot_general(
                hid_ref[...],
                source[place * shard : (place + 1) * shard, :],
                (((1,), (1,)), ((), ())),
                preferred_element_type=jnp.float32,
            )

    @pl.when(core_ref[0] == 0)
    def _():
        run(other_ref)

    @pl.when(core_ref[0] != 0)
    def _():
        run(mine_ref)

    flat = jnp.concatenate([r[...] for r in row_refs], axis=0)
    weighted = jnp.dot(high_ref[...], flat, preferred_element_type=jnp.float32)
    weighted = weighted + jnp.dot(low_ref[...], flat, preferred_element_type=jnp.float32)
    out_ref[...] = (weighted + jax.nn.sigmoid(dgate_ref[...]) * branch_ref[...]).astype(
        jnp.bfloat16
    )


def call(kernel, outs, ins, name, scratch=(), limit=LIMIT):
    return pl.pallas_call(
        kernel,
        out_shape=outs,
        in_specs=[SMEM if v.ndim == 1 and v.dtype == jnp.int32 else VMEM for v in ins],
        out_specs=jax.tree.map(lambda _: VMEM, outs),
        scratch_shapes=list(scratch),
        compiler_params=pltpu.CompilerParams(vmem_limit_bytes=limit),
        name=name,
    )(*ins)


def swapped(value, axis, offset):
    size = lax.axis_size(axis)
    return lax.ppermute(value, axis, [(i, i ^ offset) for i in range(size)])


def direct_shards(
    tokens, norm_gain, routes, route_weights, w_gate, w_up, w_down, dense_in, dense_out, dense_gate
):
    tok_rows, width = tokens.shape
    top_count = routes.shape[1]
    sources = lax.axis_size("ep")
    capacity = capacity_of(tok_rows, top_count, sources)
    rows = -(-capacity // 8) * 8
    me = lax.axis_index("ep").astype(jnp.int32).reshape(1)
    core = lax.axis_index("tp").astype(jnp.int32).reshape(1)
    bf16, f32 = jnp.bfloat16, jnp.float32
    own = (w_gate[0], w_up[0], w_down[0])
    other = tuple(swapped(w, "tp", 1) for w in own)

    route_cols = routes.T
    block = jax.ShapeDtypeStruct((rows, width), bf16)
    normed, *sends = call(
        lambda *r: pack_kernel(sources, rows, *r),
        (jax.ShapeDtypeStruct((tok_rows, width), bf16),) + (block,) * sources,
        (me, tokens, norm_gain.reshape(1, width), route_cols),
        "pack",
    )
    half = sources // 2
    groups = (
        tuple(range(half, half + half // 2)),
        tuple(range(half + half // 2, sources)),
        tuple(range(half)),
    )
    got = {}
    for group in groups:
        for k in group:
            got[k] = sends[k] if k == 0 else swapped(sends[k], "ep", k)

    held = jnp.where(core[0] == 0, dense_in, dense_out)
    order = [0]
    bit = half
    while bit:
        held = jnp.concatenate([held, swapped(held, "ep", bit)], axis=0)
        order = order + [k ^ bit for k in order]
        bit //= 2
    partner = swapped(held, "tp", 1)
    high, low = call(
        lambda *r: weigh_kernel(sources, rows, *r),
        (jax.ShapeDtypeStruct((tok_rows, sources * rows), bf16),) * 2,
        (me, route_cols, route_weights.T),
        "weigh",
    )
    dense_hidden = call(
        lambda *r: hidden_kernel(order, *r),
        jax.ShapeDtypeStruct((tok_rows, dense_in.shape[1]), bf16),
        (me, core, normed, held, partner),
        "dense_hidden",
    )
    back = {}
    for group in groups:
        outs = call(
            lambda *r, c=len(group): expert_kernel(c, rows, *r),
            (block,) * len(group),
            tuple(got[k] for k in group) + own + other,
            "expert",
        )
        for k, value in zip(group, outs):
            back[k] = value if k == 0 else swapped(value, "ep", k)
    return call(
        lambda *r: combine_kernel(sources, rows, order, *r),
        jax.ShapeDtypeStruct((tok_rows, width), bf16),
        (me, core, high, low, dense_hidden, held, partner, dense_gate.reshape(1, width))
        + tuple(back[k] for k in range(sources)),
        "combine",
        scratch=(pltpu.VMEM((tok_rows, width), f32),),
    )


def rounded_term(hidden_rows, down_rows):
    partial_value = jnp.dot(hidden_rows, down_rows, preferred_element_type=jnp.float32).astype(
        jnp.bfloat16
    )
    return lax.optimization_barrier(partial_value).astype(jnp.float32)


def general_shards(
    tokens, norm_gain, routes, route_weights, w_gate, w_up, w_down, dense_in, dense_out, dense_gate
):
    tok_rows, model_width = tokens.shape
    top_count = routes.shape[1]
    sources = lax.axis_size("ep")
    experts = sources * w_gate.shape[0]
    core_count = lax.axis_size("tp")
    capacity = capacity_of(tok_rows, top_count, experts)
    entries = tok_rows * top_count
    normed = rms_normed(tokens, norm_gain)
    flat_routes = routes.reshape(entries)
    onehot = flat_routes[:, None] == lax.broadcasted_iota(jnp.int32, (1, experts), 1)
    earlier_mask = (
        lax.broadcasted_iota(jnp.int32, (entries, entries), 0)
        > lax.broadcasted_iota(jnp.int32, (entries, entries), 1)
    ).astype(jnp.bfloat16)
    counted = jnp.dot(earlier_mask, onehot.astype(jnp.bfloat16), preferred_element_type=jnp.float32)
    slot_index = jnp.sum(jnp.where(onehot, counted, 0.0), axis=1).astype(jnp.int32)
    position = flat_routes * capacity + slot_index
    places = position[None, :] == lax.broadcasted_iota(jnp.int32, (experts * capacity, 1), 0)
    filled = jnp.any(places, axis=1)
    source_entry = jnp.sum(
        jnp.where(places, lax.broadcasted_iota(jnp.int32, (1, entries), 1), 0), axis=1
    )
    buffer = jnp.where(
        filled[:, None], normed[source_entry // top_count], jnp.zeros((), jnp.bfloat16)
    )
    buffer = buffer.reshape(experts, capacity, model_width)
    gate_w, up_w, down_w = (
        lax.all_gather(w_gate[0], "tp", axis=1, tiled=True),
        lax.all_gather(w_up[0], "tp", axis=1, tiled=True),
        lax.all_gather(w_down[0], "tp", axis=0, tiled=True),
    )
    received = lax.all_to_all(buffer, "ep", split_axis=0, concat_axis=0, tiled=True)
    slot_count = received.shape[1]
    flat_rows = received.reshape(sources * slot_count, model_width)
    hidden = clamped_unit(
        jnp.dot(flat_rows, gate_w, preferred_element_type=jnp.float32),
        jnp.dot(flat_rows, up_w, preferred_element_type=jnp.float32),
    )
    half_width = hidden.shape[1] // core_count
    summed = rounded_term(hidden[:, :half_width], down_w[:half_width])
    summed = summed + rounded_term(
        hidden[:, half_width : half_width + half_width],
        down_w[half_width : half_width + half_width],
    )
    expert_out = summed.astype(jnp.bfloat16).reshape(sources, slot_count, model_width)
    returned = lax.all_to_all(expert_out, "ep", split_axis=0, concat_axis=0, tiled=True)
    flat_returned = returned.reshape(experts * capacity, model_width)
    picked = flat_returned[position].astype(jnp.float32).reshape(tok_rows, top_count, model_width)
    weighted = jnp.sum(picked * route_weights[:, :, None], axis=1)
    whole_in, whole_out = (
        lax.all_gather(dense_in, "ep", axis=0, tiled=True),
        lax.all_gather(dense_out, "ep", axis=0, tiled=True),
    )
    dense_hidden = jax.nn.silu(
        jnp.dot(normed, whole_in, preferred_element_type=jnp.float32)
    ).astype(jnp.bfloat16)
    branch = lax.dot_general(
        dense_hidden, whole_out, (((1,), (1,)), ((), ())), preferred_element_type=jnp.float32
    )
    return (weighted + jax.nn.sigmoid(dense_gate) * branch).astype(jnp.bfloat16)


def solution(mesh):
    placed = (
        P(("ep", "tp"), None),
        P(),
        P(("ep", "tp"), None),
        P(("ep", "tp"), None),
        P("ep", None, "tp"),
        P("ep", None, "tp"),
        P("ep", "tp", None),
        P("ep", None),
        P("ep", None),
        P(),
    )

    def body(*arrays):
        tokens, routes, dense_in = arrays[0], arrays[2], arrays[7]
        sources = mesh.shape["ep"]
        capacity = capacity_of(tokens.shape[0], routes.shape[1], sources)
        direct = (
            sources & (sources - 1) == 0
            and mesh.shape["tp"] == 2
            and arrays[4].shape[0] == 1
            and capacity >= 8
            and dense_in.shape[0] % 128 == 0
        )
        return (direct_shards if direct else general_shards)(*arrays)

    return jax.shard_map(
        body, mesh=mesh, in_specs=placed, out_specs=P(("ep", "tp"), None), check_vma=False
    )
```

```python
import math

import jax
import jax.numpy as jnp
from jax import lax
from jax.experimental import pallas as pl
from jax.experimental.pallas import tpu as pltpu
from jax.sharding import PartitionSpec as P


CLAMP_LIMIT = 7.0
SLOPE_ALPHA = 1.702
NORM_EPS = 1e-06
VMEM = pl.BlockSpec(memory_space=pltpu.VMEM)
HBM = pl.BlockSpec(memory_space=pltpu.HBM)
LIMIT = 40 * 1024 * 1024


def capacity_of(tok_rows, top_count, experts):
    return (4 * tok_rows * top_count + 3 * experts - 1) // (3 * experts)


def rms_normed(tokens, norm_gain):
    widened = tokens.astype(jnp.float32)
    inv_scale = lax.rsqrt(jnp.mean(widened * widened, axis=1, keepdims=True) + NORM_EPS)
    return (widened * inv_scale * norm_gain).astype(jnp.bfloat16)


def clamped_unit(gate_pre, up_pre):
    gate_clip = jnp.minimum(gate_pre, CLAMP_LIMIT)
    up_clip = jnp.clip(up_pre, -CLAMP_LIMIT, CLAMP_LIMIT)
    return ((up_clip + 1.0) * gate_clip * jax.nn.sigmoid(SLOPE_ALPHA * gate_clip)).astype(
        jnp.bfloat16
    )


def position():
    return lax.axis_index("ep").astype(jnp.int32), lax.axis_index("tp").astype(jnp.int32)


def row_split(capacity, width):
    pieces = 8 // math.gcd(capacity, 8)
    return pieces if width % (128 * pieces) == 0 else 1


def position():
    return lax.axis_index("ep").astype(jnp.int32), lax.axis_index("tp").astype(jnp.int32)


def row_split(capacity, width):
    pieces = 8 // math.gcd(capacity, 8)
    return pieces if width % (128 * pieces) == 0 else 1


def position():
    return lax.axis_index("ep").astype(jnp.int32), lax.axis_index("tp").astype(jnp.int32)


def row_split(capacity, width):
    pieces = 8 // math.gcd(capacity, 8)
    return pieces if width % (128 * pieces) == 0 else 1


def expert_column(plan):
    me, core = position()
    block = lax.broadcasted_iota(jnp.int32, (len(plan), 1), 0)
    column = jnp.zeros((len(plan), 1), jnp.int32)
    for m, (first, second) in enumerate(plan):
        column = jnp.where(block == m, jnp.where(core == 0, first, second), column)
    return jnp.bitwise_xor(column, me)


def choice_masks(routes, expert):
    return [routes[c : c + 1, :] == expert for c in range(routes.shape[0])]


def slot_ranks(routes, expert):
    tokens = routes.shape[1]
    chosen = sum(jnp.where(mask, 1.0, 0.0) for mask in choice_masks(routes, expert))
    earlier = lax.broadcasted_iota(jnp.int32, (tokens, tokens), 0) < lax.broadcasted_iota(
        jnp.int32, (tokens, tokens), 1
    )
    counted = jnp.dot(
        chosen.astype(jnp.bfloat16),
        jnp.where(earlier, 1.0, 0.0).astype(jnp.bfloat16),
        preferred_element_type=jnp.float32,
    )
    return jnp.where(chosen > 0.0, counted, -1.0)


def block_rows(capacity, pieces):
    row = lax.broadcasted_iota(jnp.int32, (capacity * pieces, 1), 0)
    piece = sum((row >= h * capacity).astype(jnp.int32) for h in range(1, pieces)) + 0 * row
    return piece, (row - piece * capacity).astype(jnp.float32)


def load_kernel(tok_ref, gain_ref, route_ref, rate_ref, in_ref, out_ref, held_ref, norm_ref,
                gain_v, route_v, rate_v, tok_v, sems):
    _, core = position()
    pairs = ((tok_ref, tok_v), (gain_ref, gain_v), (route_ref, route_v), (rate_ref, rate_v))
    copies = [pltpu.make_async_copy(a, b, sems.at[i]) for i, (a, b) in enumerate(pairs)]
    for copy in copies:
        copy.start()
    last = sems.at[len(pairs)]

    @pl.when(core == 0)
    def _():
        pltpu.make_async_copy(in_ref, held_ref, last).start()

    @pl.when(core != 0)
    def _():
        pltpu.make_async_copy(out_ref, held_ref, last).start()

    for copy in copies:
        copy.wait()
    norm_ref[...] = rms_normed(tok_v[...], gain_v[...])
    pltpu.make_async_copy(in_ref, held_ref, last).wait()


def pack_kernel(capacity, plan, own_ref, tok2_ref, gain_ref, route_ref, route2_ref,
                norm_ref, *send_refs):
    half = own_ref.shape[0]
    rows, part = send_refs[0].shape
    pieces = rows // capacity
    norm_ref[:half, :] = own_ref[...]
    norm_ref[half:, :] = rms_normed(tok2_ref[...], gain_ref[...])
    routes = jnp.concatenate([route_ref[...], route2_ref[...]], axis=1)
    ranks = slot_ranks(routes, expert_column(plan))
    piece, slot = block_rows(capacity, pieces)
    packed = None
    for h in range(pieces):
        select = jnp.concatenate(
            [
                jnp.where((ranks[m : m + 1, :] == slot) & (piece == h), 1.0, 0.0)
                for m in range(len(send_refs))
            ],
            axis=0,
        ).astype(jnp.bfloat16)
        term = jnp.dot(
            select, norm_ref[:, h * part : (h + 1) * part], preferred_element_type=jnp.float32
        )
        packed = term if packed is None else packed + term
    packed = packed.astype(jnp.bfloat16)
    for m, send_ref in enumerate(send_refs):
        send_ref[...] = packed[m * rows : (m + 1) * rows, :]


def whole_rows(block, capacity, padded):
    rows = block.shape[0]
    pieces = rows // capacity
    if pieces == 1:
        return block
    wide = block.astype(jnp.float32)
    parts = [wide[:padded]] + [
        pltpu.roll(wide, rows - h * capacity, 0)[:padded] for h in range(1, pieces)
    ]
    return jnp.concatenate(parts, axis=1).astype(jnp.bfloat16)


def split_rows(values, capacity, pieces):
    if pieces == 1:
        return values
    rows, part = capacity * pieces, values.shape[1] // pieces
    piece, _ = block_rows(capacity, pieces)
    filler = jnp.zeros((rows - values.shape[0], part), values.dtype)
    block = None
    for h in range(pieces):
        each = jnp.concatenate([values[:, h * part : (h + 1) * part], filler], axis=0)
        block = each if h == 0 else jnp.where(piece == h, pltpu.roll(each, h * capacity, 0), block)
    return block


def expert_kernel(count, capacity, *refs):
    row_refs, refs = refs[:count], refs[count:]
    (gate0, up0, down0, gate1, up1, down1), out_refs = refs[:6], refs[6:]
    pieces = row_refs[0].shape[0] // capacity
    padded = -(-capacity // 8) * 8
    flat = jnp.concatenate([whole_rows(r[...], capacity, padded) for r in row_refs], axis=0)
    total = None
    for gate_ref, up_ref, down_ref in ((gate0, up0, down0), (gate1, up1, down1)):
        hidden = clamped_unit(
            jnp.dot(flat, gate_ref[...], preferred_element_type=jnp.float32),
            jnp.dot(flat, up_ref[...], preferred_element_type=jnp.float32),
        )
        part = jnp.dot(hidden, down_ref[...], preferred_element_type=jnp.float32)
        part = part.astype(jnp.bfloat16).astype(jnp.float32)
        total = part if total is None else total + part
    for k in range(count):
        values = total[k * padded : (k + 1) * padded, :]
        out_refs[k][...] = split_rows(values, capacity, pieces).astype(jnp.bfloat16)


def weigh_kernel(capacity, pieces, plan, early, route_ref, route2_ref, rate_ref, rate2_ref,
                 *out_refs):
    routes = jnp.concatenate([route_ref[...], route2_ref[...]], axis=1)
    weights = jnp.concatenate([rate_ref[...], rate2_ref[...]], axis=1)
    expert = expert_column(plan)
    ranks = slot_ranks(routes, expert)
    scale = sum(
        jnp.where(mask, weights[c : c + 1, :], 0.0)
        for c, mask in enumerate(choice_masks(routes, expert))
    )
    piece, slot = block_rows(capacity, pieces)
    tokens = routes.shape[1]
    tables = [
        jnp.where(ranks[m : m + 1, :] == slot, scale[m : m + 1, :], 0.0) for m in range(len(plan))
    ]
    for group, (high_ref, low_ref) in zip(
        (tables[:early], tables[early:]), (out_refs[:2], out_refs[2:])
    ):
        for h in range(pieces):
            table = jnp.concatenate([jnp.where(piece == h, t, 0.0) for t in group], axis=0).T
            high = table.astype(jnp.bfloat16)
            high_ref[h * tokens : (h + 1) * tokens, :] = high
            low_ref[h * tokens : (h + 1) * tokens, :] = (
                table - high.astype(jnp.float32)
            ).astype(jnp.bfloat16)


def join_kernel(*refs):
    at = 0
    for ref in refs[:-1]:
        refs[-1][at : at + ref.shape[0], :] = ref[...]
        at += ref.shape[0]


def shards_of(order, refs):
    place = 0
    shard = sum(r.shape[0] for r in refs) // len(order)
    for ref in refs:
        for at in range(0, ref.shape[0], shard):
            yield shard, order[place], ref, at
            place += 1


def hidden_kernel(order, norm_ref, *refs):
    held_refs, out_ref = refs[:-1], refs[-1]
    me, core = position()

    @pl.when(core == 0)
    def _():
        total = None
        for shard, offset, ref, at in shards_of(order, held_refs):
            source = pl.multiple_of(jnp.bitwise_xor(me, offset) * shard, shard)
            part = jnp.dot(
                norm_ref[:, pl.ds(source, shard)],
                ref[at : at + shard, :],
                preferred_element_type=jnp.float32,
            )
            total = part if total is None else total + part
        out_ref[...] = (total / (1.0 + jnp.exp(-total))).astype(jnp.bfloat16)

    @pl.when(core != 0)
    def _():
        out_ref[...] = jnp.zeros_like(out_ref)


def gather_into(out_ref, start_ref, row_refs, high_ref, low_ref):
    flat = jnp.concatenate([r[...] for r in row_refs], axis=0)
    tokens, part = out_ref.shape[0], flat.shape[1]
    for h in range(out_ref.shape[1] // part):
        at = slice(h * tokens, (h + 1) * tokens)
        value = jnp.dot(high_ref[at, :], flat, preferred_element_type=jnp.float32)
        value = value + jnp.dot(low_ref[at, :], flat, preferred_element_type=jnp.float32)
        lanes = slice(h * part, (h + 1) * part)
        out_ref[:, lanes] = value if start_ref is None else value + start_ref[:, lanes]


def early_kernel(order, held_count, high_ref, low_ref, hid_ref, dgate_ref, *refs):
    held_refs, row_refs, out_ref = refs[:held_count], refs[held_count:-1], refs[-1]
    me, core = position()
    gather_into(out_ref, None, row_refs, high_ref, low_ref)

    @pl.when(core != 0)
    def _():
        half = hid_ref.shape[0] // 2
        hid = jnp.concatenate([hid_ref[half:, :], hid_ref[:half, :]], axis=0)
        for shard, offset, ref, at in shards_of(order, held_refs):
            lanes = pl.ds(pl.multiple_of(jnp.bitwise_xor(me, offset) * shard, shard), shard)
            branch = lax.dot_general(
                hid,
                ref[at : at + shard, :],
                (((1,), (1,)), ((), ())),
                preferred_element_type=jnp.float32,
            )
            out_ref[:, lanes] += jax.nn.sigmoid(dgate_ref[:, lanes]) * branch


def late_kernel(early_ref, high_ref, low_ref, *refs):
    row_refs, own_ref, other_ref, sum_ref = refs[:-3], refs[-3], refs[-2], refs[-1]
    half = own_ref.shape[0]
    gather_into(sum_ref, early_ref, row_refs, high_ref, low_ref)
    own_ref[...] = sum_ref[:half, :]
    other_ref[...] = sum_ref[half:, :].astype(jnp.bfloat16)


def call(kernel, outs, ins, scratch=(), spec=VMEM):
    return pl.pallas_call(
        kernel,
        out_shape=outs,
        in_specs=[spec for _ in ins],
        out_specs=jax.tree.map(lambda _: VMEM, outs),
        scratch_shapes=list(scratch),
        compiler_params=pltpu.CompilerParams(vmem_limit_bytes=LIMIT),
    )(*ins)


def swapped(value, offsets):
    size = lax.axis_size("ep")
    pairs = [(2 * i + c, 2 * (i ^ offsets[c]) + c) for i in range(size) for c in range(2)]
    return lax.ppermute(value, ("ep", "tp"), pairs)


def partners(value):
    return lax.ppermute(value, "tp", [(0, 1), (1, 0)])


def plan_of(sources):
    half = sources // 2
    far = [(k, k + 1) for k in range(half, sources, 2)]
    near = [(k, k + 1) for k in range(0, half, 2)]
    cut = len(far) // 2
    return far[:cut] + near[1:] + near[:1] + far[cut:], cut, len(near)


def bits_of(sources):
    return [1 << b for b in range(sources.bit_length() - 2, 1, -1)]


def direct_shards(
    tokens, norm_gain, routes, route_weights, w_gate, w_up, w_down, dense_in, dense_out, dense_gate
):
    tok_rows, width = tokens.shape
    sources = lax.axis_size("ep")
    capacity = 2 * capacity_of(tok_rows, routes.shape[1], sources)
    pieces = row_split(capacity, width)
    bf16, f32 = jnp.bfloat16, jnp.float32
    shape = jax.ShapeDtypeStruct
    plan, cut, near = plan_of(sources)
    blocks = len(plan)
    early = cut + near
    groups = (range(cut, early), range(cut), range(early, blocks))

    gain = norm_gain.reshape(1, width)
    routes, rates = routes.T, route_weights.T
    tokens2 = partners(tokens)
    routes2 = partners(routes)
    rates2 = partners(rates)
    own = (w_gate[0], w_up[0], w_down[0])
    other = tuple(partners(w) for w in own)

    inputs = (tokens, gain, routes, rates)
    held, norm_own, gain, routes, rates = call(
        load_kernel,
        tuple(shape(v.shape, v.dtype) for v in (dense_in,) + inputs),
        inputs + (dense_in, dense_out),
        scratch=(pltpu.VMEM(tokens.shape, bf16), pltpu.SemaphoreType.DMA((5,))),
        spec=HBM,
    )
    block = shape((capacity * pieces, width // pieces), bf16)
    normed, *sends = call(
        lambda *r: pack_kernel(capacity, plan, *r),
        (shape((2 * tok_rows, width), bf16),) + (block,) * blocks,
        (norm_own, tokens2, gain, routes, routes2),
    )
    got = [swapped(sends[m], plan[m]) for m in range(blocks)]

    order = [0]
    for bit in bits_of(sources):
        more = swapped(held, (bit, bit))
        held = call(join_kernel, shape((2 * held.shape[0], held.shape[1]), bf16), (held, more))
        order = order + [k ^ bit for k in order]
    helds = (held,) + tuple(swapped(held, (k, k)) for k in (1, 2, 3))
    order = [k ^ j for j in range(4) for k in order]

    columns = (early * block.shape[0], (blocks - early) * block.shape[0])
    high0, low0, high1, low1 = call(
        lambda *r: weigh_kernel(capacity, pieces, plan, early, *r),
        tuple(shape((2 * tok_rows * pieces, n), bf16) for n in columns for _ in range(2)),
        (routes, routes2, rates, rates2),
    )
    dense_hidden = call(
        lambda *r: hidden_kernel(order, *r),
        shape((2 * tok_rows, dense_in.shape[1]), bf16),
        (normed,) + helds,
    )
    dense_hidden = partners(dense_hidden)
    back = {}
    for group in groups:
        outs = call(
            lambda *r, c=len(group): expert_kernel(c, capacity, *r),
            (block,) * len(group),
            tuple(got[m] for m in group) + own + other,
        )
        for m, value in zip(group, outs):
            back[m] = swapped(value, plan[m])
    sum0 = call(
        lambda *r: early_kernel(order, len(helds), *r),
        shape((2 * tok_rows, width), f32),
        (high0, low0, dense_hidden, dense_gate.reshape(1, width))
        + helds
        + tuple(back[m] for m in range(early)),
    )
    total, share = call(
        late_kernel,
        (shape((tok_rows, width), f32), shape((tok_rows, width), bf16)),
        (sum0, high1, low1) + tuple(back[m] for m in range(early, blocks)),
        scratch=(pltpu.VMEM((2 * tok_rows, width), f32),),
    )
    return (total + partners(share).astype(f32)).astype(bf16)


def rounded_term(hidden_rows, down_rows):
    partial_value = jnp.dot(hidden_rows, down_rows, preferred_element_type=jnp.float32).astype(
        jnp.bfloat16
    )
    return lax.optimization_barrier(partial_value).astype(jnp.float32)


def general_shards(
    tokens, norm_gain, routes, route_weights, w_gate, w_up, w_down, dense_in, dense_out, dense_gate
):
    tok_rows, model_width = tokens.shape
    top_count = routes.shape[1]
    sources = lax.axis_size("ep")
    experts = sources * w_gate.shape[0]
    core_count = lax.axis_size("tp")
    capacity = capacity_of(tok_rows, top_count, experts)
    entries = tok_rows * top_count
    normed = rms_normed(tokens, norm_gain)
    flat_routes = routes.reshape(entries)
    onehot = flat_routes[:, None] == lax.broadcasted_iota(jnp.int32, (1, experts), 1)
    earlier_mask = (
        lax.broadcasted_iota(jnp.int32, (entries, entries), 0)
        > lax.broadcasted_iota(jnp.int32, (entries, entries), 1)
    ).astype(jnp.bfloat16)
    counted = jnp.dot(earlier_mask, onehot.astype(jnp.bfloat16), preferred_element_type=jnp.float32)
    slot_index = jnp.sum(jnp.where(onehot, counted, 0.0), axis=1).astype(jnp.int32)
    position = flat_routes * capacity + slot_index
    places = position[None, :] == lax.broadcasted_iota(jnp.int32, (experts * capacity, 1), 0)
    filled = jnp.any(places, axis=1)
    source_entry = jnp.sum(
        jnp.where(places, lax.broadcasted_iota(jnp.int32, (1, entries), 1), 0), axis=1
    )
    buffer = jnp.where(
        filled[:, None], normed[source_entry // top_count], jnp.zeros((), jnp.bfloat16)
    )
    buffer = buffer.reshape(experts, capacity, model_width)
    gate_w, up_w, down_w = (
        lax.all_gather(w_gate[0], "tp", axis=1, tiled=True),
        lax.all_gather(w_up[0], "tp", axis=1, tiled=True),
        lax.all_gather(w_down[0], "tp", axis=0, tiled=True),
    )
    received = lax.all_to_all(buffer, "ep", split_axis=0, concat_axis=0, tiled=True)
    slot_count = received.shape[1]
    flat_rows = received.reshape(sources * slot_count, model_width)
    hidden = clamped_unit(
        jnp.dot(flat_rows, gate_w, preferred_element_type=jnp.float32),
        jnp.dot(flat_rows, up_w, preferred_element_type=jnp.float32),
    )
    half_width = hidden.shape[1] // core_count
    summed = rounded_term(hidden[:, :half_width], down_w[:half_width])
    summed = summed + rounded_term(
        hidden[:, half_width : half_width + half_width],
        down_w[half_width : half_width + half_width],
    )
    expert_out = summed.astype(jnp.bfloat16).reshape(sources, slot_count, model_width)
    returned = lax.all_to_all(expert_out, "ep", split_axis=0, concat_axis=0, tiled=True)
    flat_returned = returned.reshape(experts * capacity, model_width)
    picked = flat_returned[position].astype(jnp.float32).reshape(tok_rows, top_count, model_width)
    weighted = jnp.sum(picked * route_weights[:, :, None], axis=1)
    whole_in, whole_out = (
        lax.all_gather(dense_in, "ep", axis=0, tiled=True),
        lax.all_gather(dense_out, "ep", axis=0, tiled=True),
    )
    dense_hidden = jax.nn.silu(
        jnp.dot(normed, whole_in, preferred_element_type=jnp.float32)
    ).astype(jnp.bfloat16)
    branch = lax.dot_general(
        dense_hidden, whole_out, (((1,), (1,)), ((), ())), preferred_element_type=jnp.float32
    )
    return (weighted + jax.nn.sigmoid(dense_gate) * branch).astype(jnp.bfloat16)


def solution(mesh):
    placed = (
        P(("ep", "tp"), None),
        P(),
        P(("ep", "tp"), None),
        P(("ep", "tp"), None),
        P("ep", None, "tp"),
        P("ep", None, "tp"),
        P("ep", "tp", None),
        P("ep", None),
        P("ep", None),
        P(),
    )
    sources = mesh.shape["ep"]

    def is_direct(tokens, routes, w_gate, dense_in):
        capacity = capacity_of(tokens.shape[0] // mesh.size, routes.shape[1], sources)
        return (
            sources >= 8
            and sources & (sources - 1) == 0
            and mesh.shape["tp"] == 2
            and w_gate.shape[0] == sources
            and capacity >= 8
            and dense_in.shape[0] % (128 * sources) == 0
        )

    def mapped(shards):
        return jax.shard_map(
            shards, mesh=mesh, in_specs=placed, out_specs=P(("ep", "tp"), None), check_vma=False
        )

    def step(*arrays):
        tokens, routes, w_gate, dense_in = arrays[0], arrays[2], arrays[4], arrays[7]
        if is_direct(tokens, routes, w_gate, dense_in):
            return mapped(direct_shards)(*arrays)
        return mapped(general_shards)(*arrays)

    return step
```

```python
import math

import jax
import jax.numpy as jnp
from jax import lax
from jax.experimental import pallas as pl
from jax.experimental.pallas import tpu as pltpu
from jax.sharding import PartitionSpec as P


CLAMP_LIMIT = 7.0
SLOPE_ALPHA = 1.702
NORM_EPS = 1e-06
VMEM = pl.BlockSpec(memory_space=pltpu.VMEM)
HBM = pl.BlockSpec(memory_space=pltpu.HBM)
LIMIT = 40 * 1024 * 1024


def capacity_of(tok_rows, top_count, experts):
    return (4 * tok_rows * top_count + 3 * experts - 1) // (3 * experts)


def rms_normed(tokens, norm_gain):
    widened = tokens.astype(jnp.float32)
    inv_scale = lax.rsqrt(jnp.mean(widened * widened, axis=1, keepdims=True) + NORM_EPS)
    return (widened * inv_scale * norm_gain).astype(jnp.bfloat16)


def clamped_unit(gate_pre, up_pre):
    gate_clip = jnp.minimum(gate_pre, CLAMP_LIMIT)
    up_clip = jnp.clip(up_pre, -CLAMP_LIMIT, CLAMP_LIMIT)
    return ((up_clip + 1.0) * gate_clip * jax.nn.sigmoid(SLOPE_ALPHA * gate_clip)).astype(
        jnp.bfloat16
    )


def position():
    return lax.axis_index("ep").astype(jnp.int32), lax.axis_index("tp").astype(jnp.int32)


def row_split(capacity, width):
    pieces = 8 // math.gcd(capacity, 8)
    return pieces if width % (128 * pieces) == 0 else 1


def position():
    return lax.axis_index("ep").astype(jnp.int32), lax.axis_index("tp").astype(jnp.int32)


def row_split(capacity, width):
    pieces = 8 // math.gcd(capacity, 8)
    return pieces if width % (128 * pieces) == 0 else 1


def expert_column(plan):
    me, core = position()
    block = lax.broadcasted_iota(jnp.int32, (len(plan), 1), 0)
    column = jnp.zeros((len(plan), 1), jnp.int32)
    for m, (first, second) in enumerate(plan):
        column = jnp.where(block == m, jnp.where(core == 0, first, second), column)
    return jnp.bitwise_xor(column, me)


def choice_masks(routes, expert):
    return [routes[c : c + 1, :] == expert for c in range(routes.shape[0])]


def slot_ranks(routes, expert):
    tokens = routes.shape[1]
    chosen = sum(jnp.where(mask, 1.0, 0.0) for mask in choice_masks(routes, expert))
    earlier = lax.broadcasted_iota(jnp.int32, (tokens, tokens), 0) < lax.broadcasted_iota(
        jnp.int32, (tokens, tokens), 1
    )
    counted = jnp.dot(
        chosen.astype(jnp.bfloat16),
        jnp.where(earlier, 1.0, 0.0).astype(jnp.bfloat16),
        preferred_element_type=jnp.float32,
    )
    return jnp.where(chosen > 0.0, counted, -1.0)


def block_rows(capacity, pieces):
    row = lax.broadcasted_iota(jnp.int32, (capacity * pieces, 1), 0)
    piece = sum((row >= h * capacity).astype(jnp.int32) for h in range(1, pieces)) + 0 * row
    return piece, (row - piece * capacity).astype(jnp.float32)


def load_kernel(tok_ref, gain_ref, route_ref, rate_ref, in_ref, out_ref, held_ref, norm_ref,
                gain_v, route_v, rate_v, tok_v, sems):
    _, core = position()
    pairs = ((tok_ref, tok_v), (gain_ref, gain_v), (route_ref, route_v), (rate_ref, rate_v))
    copies = [pltpu.make_async_copy(a, b, sems.at[i]) for i, (a, b) in enumerate(pairs)]
    for copy in copies:
        copy.start()
    last = sems.at[len(pairs)]

    @pl.when(core == 0)
    def _():
        pltpu.make_async_copy(in_ref, held_ref, last).start()

    @pl.when(core != 0)
    def _():
        pltpu.make_async_copy(out_ref, held_ref, last).start()

    for copy in copies:
        copy.wait()
    norm_ref[...] = rms_normed(tok_v[...], gain_v[...])
    pltpu.make_async_copy(in_ref, held_ref, last).wait()


def pack_kernel(capacity, plan, own_ref, tok2_ref, gain_ref, route_ref, route2_ref,
                norm_ref, *send_refs):
    half = own_ref.shape[0]
    rows, part = send_refs[0].shape
    pieces = rows // capacity
    norm_ref[:half, :] = own_ref[...]
    norm_ref[half:, :] = rms_normed(tok2_ref[...], gain_ref[...])
    routes = jnp.concatenate([route_ref[...], route2_ref[...]], axis=1)
    ranks = slot_ranks(routes, expert_column(plan))
    piece, slot = block_rows(capacity, pieces)
    packed = None
    for h in range(pieces):
        select = jnp.concatenate(
            [
                jnp.where((ranks[m : m + 1, :] == slot) & (piece == h), 1.0, 0.0)
                for m in range(len(send_refs))
            ],
            axis=0,
        ).astype(jnp.bfloat16)
        term = jnp.dot(
            select, norm_ref[:, h * part : (h + 1) * part], preferred_element_type=jnp.float32
        )
        packed = term if packed is None else packed + term
    packed = packed.astype(jnp.bfloat16)
    for m, send_ref in enumerate(send_refs):
        send_ref[...] = packed[m * rows : (m + 1) * rows, :]


def whole_rows(block, capacity, padded):
    rows = block.shape[0]
    pieces = rows // capacity
    if pieces == 1:
        return block
    wide = block.astype(jnp.float32)
    parts = [wide[:padded]] + [
        pltpu.roll(wide, rows - h * capacity, 0)[:padded] for h in range(1, pieces)
    ]
    return jnp.concatenate(parts, axis=1).astype(jnp.bfloat16)


def split_rows(values, capacity, pieces):
    if pieces == 1:
        return values
    rows, part = capacity * pieces, values.shape[1] // pieces
    piece, _ = block_rows(capacity, pieces)
    filler = jnp.zeros((rows - values.shape[0], part), values.dtype)
    block = None
    for h in range(pieces):
        each = jnp.concatenate([values[:, h * part : (h + 1) * part], filler], axis=0)
        block = each if h == 0 else jnp.where(piece == h, pltpu.roll(each, h * capacity, 0), block)
    return block


def expert_kernel(count, capacity, *refs):
    row_refs, refs = refs[:count], refs[count:]
    (gate0, up0, down0, gate1, up1, down1), out_refs = refs[:6], refs[6:]
    pieces = row_refs[0].shape[0] // capacity
    padded = -(-capacity // 8) * 8
    flat = jnp.concatenate([whole_rows(r[...], capacity, padded) for r in row_refs], axis=0)
    total = None
    for gate_ref, up_ref, down_ref in ((gate0, up0, down0), (gate1, up1, down1)):
        hidden = clamped_unit(
            jnp.dot(flat, gate_ref[...], preferred_element_type=jnp.float32),
            jnp.dot(flat, up_ref[...], preferred_element_type=jnp.float32),
        )
        part = jnp.dot(hidden, down_ref[...], preferred_element_type=jnp.float32)
        part = part.astype(jnp.bfloat16).astype(jnp.float32)
        total = part if total is None else total + part
    for k in range(count):
        values = total[k * padded : (k + 1) * padded, :]
        out_refs[k][...] = split_rows(values, capacity, pieces).astype(jnp.bfloat16)


def weigh_kernel(capacity, pieces, plan, early, route_ref, route2_ref, rate_ref, rate2_ref,
                 *out_refs):
    routes = jnp.concatenate([route_ref[...], route2_ref[...]], axis=1)
    weights = jnp.concatenate([rate_ref[...], rate2_ref[...]], axis=1)
    expert = expert_column(plan)
    ranks = slot_ranks(routes, expert)
    scale = sum(
        jnp.where(mask, weights[c : c + 1, :], 0.0)
        for c, mask in enumerate(choice_masks(routes, expert))
    )
    piece, slot = block_rows(capacity, pieces)
    tokens = routes.shape[1]
    tables = [
        jnp.where(ranks[m : m + 1, :] == slot, scale[m : m + 1, :], 0.0) for m in range(len(plan))
    ]
    for group, (high_ref, low_ref) in zip(
        (tables[:early], tables[early:]), (out_refs[:2], out_refs[2:])
    ):
        for h in range(pieces):
            table = jnp.concatenate([jnp.where(piece == h, t, 0.0) for t in group], axis=0).T
            high = table.astype(jnp.bfloat16)
            high_ref[h * tokens : (h + 1) * tokens, :] = high
            low_ref[h * tokens : (h + 1) * tokens, :] = (
                table - high.astype(jnp.float32)
            ).astype(jnp.bfloat16)


def fetch_kernel(*refs):
    count = len(refs) // 2
    sems = refs[-1]
    copies = [
        pltpu.make_async_copy(refs[i].at[0], refs[count + i], sems.at[i]) for i in range(count)
    ]
    for copy in copies:
        copy.start()
    for copy in copies:
        copy.wait()


def join_kernel(*refs):
    at = 0
    for ref in refs[:-1]:
        refs[-1][at : at + ref.shape[0], :] = ref[...]
        at += ref.shape[0]


def shards_of(order, refs):
    place = 0
    shard = sum(r.shape[0] for r in refs) // len(order)
    for ref in refs:
        for at in range(0, ref.shape[0], shard):
            yield shard, order[place], ref, at
            place += 1


def hidden_kernel(order, norm_ref, *refs):
    held_refs, out_ref = refs[:-1], refs[-1]
    me, core = position()

    @pl.when(core == 0)
    def _():
        total = None
        for shard, offset, ref, at in shards_of(order, held_refs):
            source = pl.multiple_of(jnp.bitwise_xor(me, offset) * shard, shard)
            part = jnp.dot(
                norm_ref[:, pl.ds(source, shard)],
                ref[at : at + shard, :],
                preferred_element_type=jnp.float32,
            )
            total = part if total is None else total + part
        out_ref[...] = (total / (1.0 + jnp.exp(-total))).astype(jnp.bfloat16)

    @pl.when(core != 0)
    def _():
        out_ref[...] = jnp.zeros_like(out_ref)


def gather_into(out_ref, start_ref, row_refs, high_ref, low_ref):
    flat = jnp.concatenate([r[...] for r in row_refs], axis=0)
    tokens, part = out_ref.shape[0], flat.shape[1]
    for h in range(out_ref.shape[1] // part):
        at = slice(h * tokens, (h + 1) * tokens)
        value = jnp.dot(high_ref[at, :], flat, preferred_element_type=jnp.float32)
        value = value + jnp.dot(low_ref[at, :], flat, preferred_element_type=jnp.float32)
        lanes = slice(h * part, (h + 1) * part)
        out_ref[:, lanes] = value if start_ref is None else value + start_ref[:, lanes]


def early_kernel(order, held_count, high_ref, low_ref, hid_ref, dgate_ref, *refs):
    held_refs, row_refs, out_ref = refs[:held_count], refs[held_count:-1], refs[-1]
    me, core = position()
    gather_into(out_ref, None, row_refs, high_ref, low_ref)

    @pl.when(core != 0)
    def _():
        half = hid_ref.shape[0] // 2
        hid = jnp.concatenate([hid_ref[half:, :], hid_ref[:half, :]], axis=0)
        for shard, offset, ref, at in shards_of(order, held_refs):
            lanes = pl.ds(pl.multiple_of(jnp.bitwise_xor(me, offset) * shard, shard), shard)
            branch = lax.dot_general(
                hid,
                ref[at : at + shard, :],
                (((1,), (1,)), ((), ())),
                preferred_element_type=jnp.float32,
            )
            out_ref[:, lanes] += jax.nn.sigmoid(dgate_ref[:, lanes]) * branch


def late_kernel(early_ref, high_ref, low_ref, *refs):
    row_refs, own_ref, other_ref, sum_ref = refs[:-3], refs[-3], refs[-2], refs[-1]
    half = own_ref.shape[0]
    gather_into(sum_ref, early_ref, row_refs, high_ref, low_ref)
    own_ref[...] = sum_ref[:half, :]
    other_ref[...] = sum_ref[half:, :].astype(jnp.bfloat16)


def call(kernel, outs, ins, scratch=(), spec=VMEM):
    if spec is HBM:
        ins = tuple(pltpu.with_memory_space_constraint(v, pltpu.HBM) for v in ins)
    return pl.pallas_call(
        kernel,
        out_shape=outs,
        in_specs=[spec for _ in ins],
        out_specs=jax.tree.map(lambda _: VMEM, outs),
        scratch_shapes=list(scratch),
        compiler_params=pltpu.CompilerParams(vmem_limit_bytes=LIMIT),
    )(*ins)


def swapped(value, offsets):
    size = lax.axis_size("ep")
    pairs = [(2 * i + c, 2 * (i ^ offsets[c]) + c) for i in range(size) for c in range(2)]
    return lax.ppermute(value, ("ep", "tp"), pairs)


def partners(value):
    return lax.ppermute(value, "tp", [(0, 1), (1, 0)])


def plan_of(sources):
    half = sources // 2
    far = [(k, k + 1) for k in range(half, sources, 2)]
    near = [(k, k + 1) for k in range(0, half, 2)]
    cut = len(far) // 2
    return far[:cut] + near[1:] + near[:1] + far[cut:], cut, len(near)


def bits_of(sources):
    return [1 << b for b in range(sources.bit_length() - 2, 1, -1)]


def direct_shards(
    tokens, norm_gain, routes, route_weights, w_gate, w_up, w_down, dense_in, dense_out, dense_gate
):
    tok_rows, width = tokens.shape
    sources = lax.axis_size("ep")
    capacity = 2 * capacity_of(tok_rows, routes.shape[1], sources)
    pieces = row_split(capacity, width)
    bf16, f32 = jnp.bfloat16, jnp.float32
    shape = jax.ShapeDtypeStruct
    plan, cut, near = plan_of(sources)
    blocks = len(plan)
    early = cut + near
    groups = (range(cut, early), range(cut), range(early, blocks))

    gain = norm_gain.reshape(1, width)
    routes, rates = routes.T, route_weights.T
    tokens2 = partners(tokens)
    routes2 = partners(routes)
    rates2 = partners(rates)
    own = (w_gate, w_up, w_down)
    other = tuple(partners(w[0]) for w in own)
    own = call(
        fetch_kernel,
        tuple(shape(w.shape[1:], w.dtype) for w in own),
        own,
        scratch=(pltpu.SemaphoreType.DMA((3,)),),
        spec=HBM,
    )

    inputs = (tokens, gain, routes, rates)
    held, norm_own, gain, routes, rates = call(
        load_kernel,
        tuple(shape(v.shape, v.dtype) for v in (dense_in,) + inputs),
        inputs + (dense_in, dense_out),
        scratch=(pltpu.VMEM(tokens.shape, bf16), pltpu.SemaphoreType.DMA((5,))),
        spec=HBM,
    )
    block = shape((capacity * pieces, width // pieces), bf16)
    normed, *sends = call(
        lambda *r: pack_kernel(capacity, plan, *r),
        (shape((2 * tok_rows, width), bf16),) + (block,) * blocks,
        (norm_own, tokens2, gain, routes, routes2),
    )
    got = [swapped(sends[m], plan[m]) for m in range(blocks)]

    order = [0]
    for bit in bits_of(sources):
        more = swapped(held, (bit, bit))
        held = call(join_kernel, shape((2 * held.shape[0], held.shape[1]), bf16), (held, more))
        order = order + [k ^ bit for k in order]
    helds = (held,) + tuple(swapped(held, (k, k)) for k in (1, 2, 3))
    order = [k ^ j for j in range(4) for k in order]

    columns = (early * block.shape[0], (blocks - early) * block.shape[0])
    high0, low0, high1, low1 = call(
        lambda *r: weigh_kernel(capacity, pieces, plan, early, *r),
        tuple(shape((2 * tok_rows * pieces, n), bf16) for n in columns for _ in range(2)),
        (routes, routes2, rates, rates2),
    )
    dense_hidden = call(
        lambda *r: hidden_kernel(order, *r),
        shape((2 * tok_rows, dense_in.shape[1]), bf16),
        (normed,) + helds,
    )
    dense_hidden = partners(dense_hidden)
    back = {}
    for group in groups:
        outs = call(
            lambda *r, c=len(group): expert_kernel(c, capacity, *r),
            (block,) * len(group),
            tuple(got[m] for m in group) + own + other,
        )
        for m, value in zip(group, outs):
            back[m] = swapped(value, plan[m])
    sum0 = call(
        lambda *r: early_kernel(order, len(helds), *r),
        shape((2 * tok_rows, width), f32),
        (high0, low0, dense_hidden, dense_gate.reshape(1, width))
        + helds
        + tuple(back[m] for m in range(early)),
    )
    total, share = call(
        late_kernel,
        (shape((tok_rows, width), f32), shape((tok_rows, width), bf16)),
        (sum0, high1, low1) + tuple(back[m] for m in range(early, blocks)),
        scratch=(pltpu.VMEM((2 * tok_rows, width), f32),),
    )
    return (total + partners(share).astype(f32)).astype(bf16)


def rounded_term(hidden_rows, down_rows):
    partial_value = jnp.dot(hidden_rows, down_rows, preferred_element_type=jnp.float32).astype(
        jnp.bfloat16
    )
    return lax.optimization_barrier(partial_value).astype(jnp.float32)


def general_shards(
    tokens, norm_gain, routes, route_weights, w_gate, w_up, w_down, dense_in, dense_out, dense_gate
):
    tok_rows, model_width = tokens.shape
    top_count = routes.shape[1]
    sources = lax.axis_size("ep")
    experts = sources * w_gate.shape[0]
    core_count = lax.axis_size("tp")
    capacity = capacity_of(tok_rows, top_count, experts)
    entries = tok_rows * top_count
    normed = rms_normed(tokens, norm_gain)
    flat_routes = routes.reshape(entries)
    onehot = flat_routes[:, None] == lax.broadcasted_iota(jnp.int32, (1, experts), 1)
    earlier_mask = (
        lax.broadcasted_iota(jnp.int32, (entries, entries), 0)
        > lax.broadcasted_iota(jnp.int32, (entries, entries), 1)
    ).astype(jnp.bfloat16)
    counted = jnp.dot(earlier_mask, onehot.astype(jnp.bfloat16), preferred_element_type=jnp.float32)
    slot_index = jnp.sum(jnp.where(onehot, counted, 0.0), axis=1).astype(jnp.int32)
    position = flat_routes * capacity + slot_index
    places = position[None, :] == lax.broadcasted_iota(jnp.int32, (experts * capacity, 1), 0)
    filled = jnp.any(places, axis=1)
    source_entry = jnp.sum(
        jnp.where(places, lax.broadcasted_iota(jnp.int32, (1, entries), 1), 0), axis=1
    )
    buffer = jnp.where(
        filled[:, None], normed[source_entry // top_count], jnp.zeros((), jnp.bfloat16)
    )
    buffer = buffer.reshape(experts, capacity, model_width)
    gate_w, up_w, down_w = (
        lax.all_gather(w_gate[0], "tp", axis=1, tiled=True),
        lax.all_gather(w_up[0], "tp", axis=1, tiled=True),
        lax.all_gather(w_down[0], "tp", axis=0, tiled=True),
    )
    received = lax.all_to_all(buffer, "ep", split_axis=0, concat_axis=0, tiled=True)
    slot_count = received.shape[1]
    flat_rows = received.reshape(sources * slot_count, model_width)
    hidden = clamped_unit(
        jnp.dot(flat_rows, gate_w, preferred_element_type=jnp.float32),
        jnp.dot(flat_rows, up_w, preferred_element_type=jnp.float32),
    )
    half_width = hidden.shape[1] // core_count
    summed = rounded_term(hidden[:, :half_width], down_w[:half_width])
    summed = summed + rounded_term(
        hidden[:, half_width : half_width + half_width],
        down_w[half_width : half_width + half_width],
    )
    expert_out = summed.astype(jnp.bfloat16).reshape(sources, slot_count, model_width)
    returned = lax.all_to_all(expert_out, "ep", split_axis=0, concat_axis=0, tiled=True)
    flat_returned = returned.reshape(experts * capacity, model_width)
    picked = flat_returned[position].astype(jnp.float32).reshape(tok_rows, top_count, model_width)
    weighted = jnp.sum(picked * route_weights[:, :, None], axis=1)
    whole_in, whole_out = (
        lax.all_gather(dense_in, "ep", axis=0, tiled=True),
        lax.all_gather(dense_out, "ep", axis=0, tiled=True),
    )
    dense_hidden = jax.nn.silu(
        jnp.dot(normed, whole_in, preferred_element_type=jnp.float32)
    ).astype(jnp.bfloat16)
    branch = lax.dot_general(
        dense_hidden, whole_out, (((1,), (1,)), ((), ())), preferred_element_type=jnp.float32
    )
    return (weighted + jax.nn.sigmoid(dense_gate) * branch).astype(jnp.bfloat16)


def solution(mesh):
    placed = (
        P(("ep", "tp"), None),
        P(),
        P(("ep", "tp"), None),
        P(("ep", "tp"), None),
        P("ep", None, "tp"),
        P("ep", None, "tp"),
        P("ep", "tp", None),
        P("ep", None),
        P("ep", None),
        P(),
    )
    sources = mesh.shape["ep"]

    def is_direct(tokens, routes, w_gate, dense_in):
        capacity = capacity_of(tokens.shape[0] // mesh.size, routes.shape[1], sources)
        return (
            sources >= 8
            and sources & (sources - 1) == 0
            and mesh.shape["tp"] == 2
            and w_gate.shape[0] == sources
            and capacity >= 8
            and dense_in.shape[0] % (128 * sources) == 0
        )

    def mapped(shards):
        return jax.shard_map(
            shards, mesh=mesh, in_specs=placed, out_specs=P(("ep", "tp"), None), check_vma=False
        )

    def step(*arrays):
        tokens, routes, w_gate, dense_in = arrays[0], arrays[2], arrays[4], arrays[7]
        if is_direct(tokens, routes, w_gate, dense_in):
            return mapped(direct_shards)(*arrays)
        return mapped(general_shards)(*arrays)

    return step
```

```python
import math

import jax
import jax.numpy as jnp
from jax import lax
from jax.experimental import pallas as pl
from jax.experimental.pallas import tpu as pltpu
from jax.sharding import PartitionSpec as P


CLAMP_LIMIT = 7.0
SLOPE_ALPHA = 1.702
NORM_EPS = 1e-06
VMEM = pl.BlockSpec(memory_space=pltpu.VMEM)
HBM = pl.BlockSpec(memory_space=pltpu.HBM)
LIMIT = 40 * 1024 * 1024


def capacity_of(tok_rows, top_count, experts):
    return (4 * tok_rows * top_count + 3 * experts - 1) // (3 * experts)


def rms_normed(tokens, norm_gain):
    widened = tokens.astype(jnp.float32)
    inv_scale = lax.rsqrt(jnp.mean(widened * widened, axis=1, keepdims=True) + NORM_EPS)
    return (widened * inv_scale * norm_gain).astype(jnp.bfloat16)


def clamped_unit(gate_pre, up_pre):
    gate_clip = jnp.minimum(gate_pre, CLAMP_LIMIT)
    up_clip = jnp.clip(up_pre, -CLAMP_LIMIT, CLAMP_LIMIT)
    return ((up_clip + 1.0) * gate_clip * jax.nn.sigmoid(SLOPE_ALPHA * gate_clip)).astype(
        jnp.bfloat16
    )


def position():
    return lax.axis_index("ep").astype(jnp.int32), lax.axis_index("tp").astype(jnp.int32)


def row_split(capacity, width):
    pieces = 8 // math.gcd(capacity, 8)
    return pieces if width % (128 * pieces) == 0 else 1


def position():
    return lax.axis_index("ep").astype(jnp.int32), lax.axis_index("tp").astype(jnp.int32)


def row_split(capacity, width):
    pieces = 8 // math.gcd(capacity, 8)
    return pieces if width % (128 * pieces) == 0 else 1


def expert_column(plan):
    me, core = position()
    block = lax.broadcasted_iota(jnp.int32, (len(plan), 1), 0)
    column = jnp.zeros((len(plan), 1), jnp.int32)
    for m, (first, second) in enumerate(plan):
        column = jnp.where(block == m, jnp.where(core == 0, first, second), column)
    return jnp.bitwise_xor(column, me)


def choice_masks(routes, expert):
    return [routes[c : c + 1, :] == expert for c in range(routes.shape[0])]


def slot_ranks(routes, expert, capacity):
    tokens = routes.shape[1]
    chosen = sum(jnp.where(mask, 1.0, 0.0) for mask in choice_masks(routes, expert))
    half = tokens // 2 if capacity else tokens
    row = lax.broadcasted_iota(jnp.int32, (tokens, tokens), 0)
    column = lax.broadcasted_iota(jnp.int32, (tokens, tokens), 1)
    earlier = (row < column) & ((row >= half) == (column >= half))
    counted = jnp.dot(
        chosen.astype(jnp.bfloat16),
        jnp.where(earlier, 1.0, 0.0).astype(jnp.bfloat16),
        preferred_element_type=jnp.float32,
    )
    second = lax.broadcasted_iota(jnp.int32, (1, tokens), 1) >= half
    counted = counted + jnp.where(second, float(capacity), 0.0)
    return jnp.where(chosen > 0.0, counted, -1.0)


def block_rows(capacity, pieces):
    row = lax.broadcasted_iota(jnp.int32, (capacity * pieces, 1), 0)
    piece = sum((row >= h * capacity).astype(jnp.int32) for h in range(1, pieces)) + 0 * row
    return piece, (row - piece * capacity).astype(jnp.float32)


def load_kernel(tok_ref, gain_ref, route_ref, rate_ref, in_ref, out_ref, held_ref, norm_ref,
                gain_v, route_v, rate_v, tok_v, sems):
    _, core = position()
    pairs = ((tok_ref, tok_v), (gain_ref, gain_v), (route_ref, route_v), (rate_ref, rate_v))
    copies = [pltpu.make_async_copy(a, b, sems.at[i]) for i, (a, b) in enumerate(pairs)]
    for copy in copies:
        copy.start()
    last = sems.at[len(pairs)]

    @pl.when(core == 0)
    def _():
        pltpu.make_async_copy(in_ref, held_ref, last).start()

    @pl.when(core != 0)
    def _():
        pltpu.make_async_copy(out_ref, held_ref, last).start()

    for copy in copies:
        copy.wait()
    norm_ref[...] = rms_normed(tok_v[...], gain_v[...])
    pltpu.make_async_copy(in_ref, held_ref, last).wait()


def pack_kernel(capacity, plan, own_ref, tok2_ref, gain_ref, route_ref, route2_ref,
                norm_ref, *send_refs):
    half = own_ref.shape[0]
    rows, part = send_refs[0].shape
    pieces = rows // capacity
    norm_ref[:half, :] = own_ref[...]
    norm_ref[half:, :] = rms_normed(tok2_ref[...], gain_ref[...])
    routes = jnp.concatenate([route_ref[...], route2_ref[...]], axis=1)
    ranks = slot_ranks(routes, expert_column(plan), capacity // 2)
    piece, slot = block_rows(capacity, pieces)
    packed = None
    for h in range(pieces):
        select = jnp.concatenate(
            [
                jnp.where((ranks[m : m + 1, :] == slot) & (piece == h), 1.0, 0.0)
                for m in range(len(send_refs))
            ],
            axis=0,
        ).astype(jnp.bfloat16)
        term = jnp.dot(
            select, norm_ref[:, h * part : (h + 1) * part], preferred_element_type=jnp.float32
        )
        packed = term if packed is None else packed + term
    packed = packed.astype(jnp.bfloat16)
    for m, send_ref in enumerate(send_refs):
        send_ref[...] = packed[m * rows : (m + 1) * rows, :]


def whole_rows(block, capacity, padded):
    rows = block.shape[0]
    pieces = rows // capacity
    if pieces == 1:
        return block
    wide = block.astype(jnp.float32)
    parts = [wide[:padded]] + [
        pltpu.roll(wide, rows - h * capacity, 0)[:padded] for h in range(1, pieces)
    ]
    return jnp.concatenate(parts, axis=1).astype(jnp.bfloat16)


def split_rows(values, capacity, pieces):
    if pieces == 1:
        return values
    rows, part = capacity * pieces, values.shape[1] // pieces
    piece, _ = block_rows(capacity, pieces)
    filler = jnp.zeros((rows - values.shape[0], part), values.dtype)
    block = None
    for h in range(pieces):
        each = jnp.concatenate([values[:, h * part : (h + 1) * part], filler], axis=0)
        block = each if h == 0 else jnp.where(piece == h, pltpu.roll(each, h * capacity, 0), block)
    return block


def expert_kernel(count, capacity, halves, *refs):
    row_refs, refs = refs[:count], refs[count:]
    (gate0, up0, down0, gate1, up1, down1), out_refs = refs[:6], refs[6:]
    padded = -(-capacity // 8) * 8
    flat = jnp.concatenate([whole_rows(r[...], capacity, padded) for r in row_refs], axis=0)
    total = None
    for gate_ref, up_ref, down_ref in ((gate0, up0, down0), (gate1, up1, down1)):
        hidden = clamped_unit(
            jnp.dot(flat, gate_ref[...], preferred_element_type=jnp.float32),
            jnp.dot(flat, up_ref[...], preferred_element_type=jnp.float32),
        )
        part = jnp.dot(hidden, down_ref[...], preferred_element_type=jnp.float32)
        part = part.astype(jnp.bfloat16).astype(jnp.float32)
        total = part if total is None else total + part
    for k in range(count):
        values = total[k * padded : (k + 1) * padded, :]
        share = capacity // halves
        for j in range(halves):
            out_ref = out_refs[k * halves + j]
            part = values if j == 0 else pltpu.roll(values, padded - j * share, 0)
            part = part[: -(-share // 8) * 8]
            out_ref[...] = split_rows(part, share, out_ref.shape[0] // share).astype(jnp.bfloat16)


def weigh_kernel(capacity, pieces, plan, *refs):
    count = (len(refs) - 2) // 2
    high_ref, low_ref = refs[-2:]
    routes = jnp.concatenate([r[...] for r in refs[:count]], axis=1)
    weights = jnp.concatenate([r[...] for r in refs[count : 2 * count]], axis=1)
    expert = expert_column(plan)
    ranks = slot_ranks(routes, expert, capacity // 2 if count == 2 else 0)
    scale = sum(
        jnp.where(mask, weights[c : c + 1, :], 0.0)
        for c, mask in enumerate(choice_masks(routes, expert))
    )
    piece, slot = block_rows(capacity, pieces)
    tokens = routes.shape[1]
    tables = [
        jnp.where(ranks[m : m + 1, :] == slot, scale[m : m + 1, :], 0.0) for m in range(len(plan))
    ]
    for h in range(pieces):
        table = jnp.concatenate([jnp.where(piece == h, t, 0.0) for t in tables], axis=0).T
        high = table.astype(jnp.bfloat16)
        high_ref[h * tokens : (h + 1) * tokens, :] = high
        low_ref[h * tokens : (h + 1) * tokens, :] = (
            table - high.astype(jnp.float32)
        ).astype(jnp.bfloat16)


def fetch_kernel(*refs):
    count = len(refs) // 2
    sems = refs[-1]
    copies = [
        pltpu.make_async_copy(refs[i].at[0], refs[count + i], sems.at[i]) for i in range(count)
    ]
    for copy in copies:
        copy.start()
    for copy in copies:
        copy.wait()


def join_kernel(*refs):
    at = 0
    for ref in refs[:-1]:
        refs[-1][at : at + ref.shape[0], :] = ref[...]
        at += ref.shape[0]


def shards_of(order, refs):
    place = 0
    shard = sum(r.shape[0] for r in refs) // len(order)
    for ref in refs:
        for at in range(0, ref.shape[0], shard):
            yield shard, order[place], ref, at
            place += 1


def hidden_kernel(order, norm_ref, *refs):
    held_refs, out_ref = refs[:-1], refs[-1]
    me, core = position()

    @pl.when(core == 0)
    def _():
        total = None
        for shard, offset, ref, at in shards_of(order, held_refs):
            source = pl.multiple_of(jnp.bitwise_xor(me, offset) * shard, shard)
            part = jnp.dot(
                norm_ref[:, pl.ds(source, shard)],
                ref[at : at + shard, :],
                preferred_element_type=jnp.float32,
            )
            total = part if total is None else total + part
        out_ref[...] = (total / (1.0 + jnp.exp(-total))).astype(jnp.bfloat16)

    @pl.when(core != 0)
    def _():
        out_ref[...] = jnp.zeros_like(out_ref)


def gathered(row_refs, high_ref, low_ref, tokens):
    flat = jnp.concatenate([r[...] for r in row_refs], axis=0)
    part = flat.shape[1]
    for h in range(high_ref.shape[0] // tokens):
        at = slice(h * tokens, (h + 1) * tokens)
        value = jnp.dot(high_ref[at, :], flat, preferred_element_type=jnp.float32)
        value = value + jnp.dot(low_ref[at, :], flat, preferred_element_type=jnp.float32)
        yield slice(h * part, (h + 1) * part), value


def early_kernel(order, held_count, high_ref, low_ref, hid_ref, dgate_ref, *refs):
    held_refs, row_refs = refs[:held_count], refs[held_count:-3]
    own_ref, other_ref, sum_ref = refs[-3:]
    me, core = position()
    half = own_ref.shape[0]
    for lanes, value in gathered(row_refs, high_ref, low_ref, 2 * half):
        sum_ref[:, lanes] = value

    @pl.when(core != 0)
    def _():
        hid = jnp.concatenate([hid_ref[half:, :], hid_ref[:half, :]], axis=0)
        for shard, offset, ref, at in shards_of(order, held_refs):
            lanes = pl.ds(pl.multiple_of(jnp.bitwise_xor(me, offset) * shard, shard), shard)
            branch = lax.dot_general(
                hid,
                ref[at : at + shard, :],
                (((1,), (1,)), ((), ())),
                preferred_element_type=jnp.float32,
            )
            sum_ref[:, lanes] += jax.nn.sigmoid(dgate_ref[:, lanes]) * branch

    own_ref[...] = sum_ref[:half, :]
    other_ref[...] = sum_ref[half:, :].astype(jnp.bfloat16)


def late_kernel(own_ref, share_ref, high_ref, low_ref, *refs):
    row_refs, out_ref = refs[:-1], refs[-1]
    for lanes, value in gathered(row_refs, high_ref, low_ref, own_ref.shape[0]):
        value = value + (own_ref[:, lanes] + share_ref[:, lanes].astype(jnp.float32))
        out_ref[:, lanes] = value.astype(jnp.bfloat16)


def call(kernel, outs, ins, scratch=(), spec=VMEM):
    if spec is HBM:
        ins = tuple(pltpu.with_memory_space_constraint(v, pltpu.HBM) for v in ins)
    return pl.pallas_call(
        kernel,
        out_shape=outs,
        in_specs=[spec for _ in ins],
        out_specs=jax.tree.map(lambda _: VMEM, outs),
        scratch_shapes=list(scratch),
        compiler_params=pltpu.CompilerParams(vmem_limit_bytes=LIMIT),
    )(*ins)


def swapped(value, offsets, cross=0):
    size = lax.axis_size("ep")
    pairs = [(2 * i + c, 2 * (i ^ offsets[c]) + (c ^ cross)) for i in range(size) for c in range(2)]
    return lax.ppermute(value, ("ep", "tp"), pairs)


def partners(value):
    return lax.ppermute(value, "tp", [(0, 1), (1, 0)])


def plan_of(sources):
    half = sources // 2
    far = [(k, k + 1) for k in range(half, sources, 2)]
    parts = (far[: len(far) // 2], [(2, 3), (0, 1)], [(k, k + 1) for k in range(4, half, 2)],
             far[len(far) // 2 :])
    plan, groups = [], []
    for part in parts:
        groups.append(list(range(len(plan), len(plan) + len(part))))
        plan += part
    return plan, groups


def bits_of(sources):
    return [1 << b for b in range(sources.bit_length() - 2, 1, -1)]


def direct_shards(
    tokens, norm_gain, routes, route_weights, w_gate, w_up, w_down, dense_in, dense_out, dense_gate
):
    tok_rows, width = tokens.shape
    sources = lax.axis_size("ep")
    own_capacity = capacity_of(tok_rows, routes.shape[1], sources)
    capacity = 2 * own_capacity
    pieces, own_pieces = row_split(capacity, width), row_split(own_capacity, width)
    bf16, f32 = jnp.bfloat16, jnp.float32
    shape = jax.ShapeDtypeStruct
    plan, (far, plane, near, last) = plan_of(sources)
    blocks = len(plan)
    direct = near + last
    homes = [offsets for m in direct for offsets in (plan[m], plan[m][::-1])]
    early = far + plane

    gain = norm_gain.reshape(1, width)
    routes, rates = routes.T, route_weights.T
    tokens2 = partners(tokens)
    routes2 = partners(routes)
    rates2 = partners(rates)
    own = (w_gate, w_up, w_down)
    other = tuple(partners(w[0]) for w in own)
    own = call(
        fetch_kernel,
        tuple(shape(w.shape[1:], w.dtype) for w in own),
        own,
        scratch=(pltpu.SemaphoreType.DMA((3,)),),
        spec=HBM,
    )

    inputs = (tokens, gain, routes, rates)
    held, norm_own, gain, routes, rates = call(
        load_kernel,
        tuple(shape(v.shape, v.dtype) for v in (dense_in,) + inputs),
        inputs + (dense_in, dense_out),
        scratch=(pltpu.VMEM(tokens.shape, bf16), pltpu.SemaphoreType.DMA((5,))),
        spec=HBM,
    )
    block = shape((capacity * pieces, width // pieces), bf16)
    normed, *sends = call(
        lambda *r: pack_kernel(capacity, plan, *r),
        (shape((2 * tok_rows, width), bf16),) + (block,) * blocks,
        (norm_own, tokens2, gain, routes, routes2),
    )
    got = [swapped(sends[m], plan[m]) for m in range(blocks)]

    order = [0]
    for bit in bits_of(sources):
        more = swapped(held, (bit, bit))
        held = call(join_kernel, shape((2 * held.shape[0], held.shape[1]), bf16), (held, more))
        order = order + [k ^ bit for k in order]
    helds = (held,) + tuple(swapped(held, (k, k)) for k in (1, 2, 3))
    order = [k ^ j for j in range(4) for k in order]

    high, low = call(
        lambda *r: weigh_kernel(capacity, pieces, [plan[m] for m in early], *r),
        (shape((2 * tok_rows * pieces, len(early) * block.shape[0]), bf16),) * 2,
        (routes, routes2, rates, rates2),
    )
    own_block = shape((own_capacity * own_pieces, width // own_pieces), bf16)
    own_high, own_low = call(
        lambda *r: weigh_kernel(own_capacity, own_pieces, homes, *r),
        (shape((tok_rows * own_pieces, len(homes) * own_block.shape[0]), bf16),) * 2,
        (routes, rates),
    )
    dense_hidden = call(
        lambda *r: hidden_kernel(order, *r),
        shape((2 * tok_rows, dense_in.shape[1]), bf16),
        (normed,) + helds,
    )
    dense_hidden = partners(dense_hidden)
    back = {}
    for group in (plane, far, near, last):
        halves = 2 if group and group[0] in direct else 1
        outs = call(
            lambda *r, c=len(group), h=halves: expert_kernel(c, capacity, h, *r),
            (own_block if halves == 2 else block,) * (len(group) * halves),
            tuple(got[m] for m in group) + own + other,
        ) if group else ()
        for i, value in enumerate(outs):
            m, cross = group[i // halves], i % halves
            back[m, cross] = swapped(value, plan[m], cross)
    total, share = call(
        lambda *r: early_kernel(order, len(helds), *r),
        (shape((tok_rows, width), f32), shape((tok_rows, width), bf16)),
        (high, low, dense_hidden, dense_gate.reshape(1, width))
        + helds
        + tuple(back[m, 0] for m in early),
        scratch=(pltpu.VMEM((2 * tok_rows, width), f32),),
    )
    share = partners(share)
    return call(
        late_kernel,
        shape((tok_rows, width), bf16),
        (total, share, own_high, own_low) + tuple(back[m, c] for m in direct for c in range(2)),
    )


def rounded_term(hidden_rows, down_rows):
    partial_value = jnp.dot(hidden_rows, down_rows, preferred_element_type=jnp.float32).astype(
        jnp.bfloat16
    )
    return lax.optimization_barrier(partial_value).astype(jnp.float32)


def general_shards(
    tokens, norm_gain, routes, route_weights, w_gate, w_up, w_down, dense_in, dense_out, dense_gate
):
    tok_rows, model_width = tokens.shape
    top_count = routes.shape[1]
    sources = lax.axis_size("ep")
    experts = sources * w_gate.shape[0]
    core_count = lax.axis_size("tp")
    capacity = capacity_of(tok_rows, top_count, experts)
    entries = tok_rows * top_count
    normed = rms_normed(tokens, norm_gain)
    flat_routes = routes.reshape(entries)
    onehot = flat_routes[:, None] == lax.broadcasted_iota(jnp.int32, (1, experts), 1)
    earlier_mask = (
        lax.broadcasted_iota(jnp.int32, (entries, entries), 0)
        > lax.broadcasted_iota(jnp.int32, (entries, entries), 1)
    ).astype(jnp.bfloat16)
    counted = jnp.dot(earlier_mask, onehot.astype(jnp.bfloat16), preferred_element_type=jnp.float32)
    slot_index = jnp.sum(jnp.where(onehot, counted, 0.0), axis=1).astype(jnp.int32)
    position = flat_routes * capacity + slot_index
    places = position[None, :] == lax.broadcasted_iota(jnp.int32, (experts * capacity, 1), 0)
    filled = jnp.any(places, axis=1)
    source_entry = jnp.sum(
        jnp.where(places, lax.broadcasted_iota(jnp.int32, (1, entries), 1), 0), axis=1
    )
    buffer = jnp.where(
        filled[:, None], normed[source_entry // top_count], jnp.zeros((), jnp.bfloat16)
    )
    buffer = buffer.reshape(experts, capacity, model_width)
    gate_w, up_w, down_w = (
        lax.all_gather(w_gate[0], "tp", axis=1, tiled=True),
        lax.all_gather(w_up[0], "tp", axis=1, tiled=True),
        lax.all_gather(w_down[0], "tp", axis=0, tiled=True),
    )
    received = lax.all_to_all(buffer, "ep", split_axis=0, concat_axis=0, tiled=True)
    slot_count = received.shape[1]
    flat_rows = received.reshape(sources * slot_count, model_width)
    hidden = clamped_unit(
        jnp.dot(flat_rows, gate_w, preferred_element_type=jnp.float32),
        jnp.dot(flat_rows, up_w, preferred_element_type=jnp.float32),
    )
    half_width = hidden.shape[1] // core_count
    summed = rounded_term(hidden[:, :half_width], down_w[:half_width])
    summed = summed + rounded_term(
        hidden[:, half_width : half_width + half_width],
        down_w[half_width : half_width + half_width],
    )
    expert_out = summed.astype(jnp.bfloat16).reshape(sources, slot_count, model_width)
    returned = lax.all_to_all(expert_out, "ep", split_axis=0, concat_axis=0, tiled=True)
    flat_returned = returned.reshape(experts * capacity, model_width)
    picked = flat_returned[position].astype(jnp.float32).reshape(tok_rows, top_count, model_width)
    weighted = jnp.sum(picked * route_weights[:, :, None], axis=1)
    whole_in, whole_out = (
        lax.all_gather(dense_in, "ep", axis=0, tiled=True),
        lax.all_gather(dense_out, "ep", axis=0, tiled=True),
    )
    dense_hidden = jax.nn.silu(
        jnp.dot(normed, whole_in, preferred_element_type=jnp.float32)
    ).astype(jnp.bfloat16)
    branch = lax.dot_general(
        dense_hidden, whole_out, (((1,), (1,)), ((), ())), preferred_element_type=jnp.float32
    )
    return (weighted + jax.nn.sigmoid(dense_gate) * branch).astype(jnp.bfloat16)


def solution(mesh):
    placed = (
        P(("ep", "tp"), None),
        P(),
        P(("ep", "tp"), None),
        P(("ep", "tp"), None),
        P("ep", None, "tp"),
        P("ep", None, "tp"),
        P("ep", "tp", None),
        P("ep", None),
        P("ep", None),
        P(),
    )
    sources = mesh.shape["ep"]

    def is_direct(tokens, routes, w_gate, dense_in):
        capacity = capacity_of(tokens.shape[0] // mesh.size, routes.shape[1], sources)
        return (
            sources >= 8
            and sources & (sources - 1) == 0
            and mesh.shape["tp"] == 2
            and w_gate.shape[0] == sources
            and capacity >= 8
            and dense_in.shape[0] % (128 * sources) == 0
        )

    def mapped(shards):
        return jax.shard_map(
            shards, mesh=mesh, in_specs=placed, out_specs=P(("ep", "tp"), None), check_vma=False
        )

    def step(*arrays):
        tokens, routes, w_gate, dense_in = arrays[0], arrays[2], arrays[4], arrays[7]
        if is_direct(tokens, routes, w_gate, dense_in):
            return mapped(direct_shards)(*arrays)
        return mapped(general_shards)(*arrays)

    return step
```

```python
import math

import jax
import jax.numpy as jnp
from jax import lax
from jax.experimental import pallas as pl
from jax.experimental.pallas import tpu as pltpu
from jax.sharding import PartitionSpec as P


CLAMP_LIMIT = 7.0
SLOPE_ALPHA = 1.702
NORM_EPS = 1e-06
VMEM = pl.BlockSpec(memory_space=pltpu.VMEM)
HBM = pl.BlockSpec(memory_space=pltpu.HBM)
LIMIT = 40 * 1024 * 1024


def capacity_of(tok_rows, top_count, experts):
    return (4 * tok_rows * top_count + 3 * experts - 1) // (3 * experts)


def rms_normed(tokens, norm_gain):
    widened = tokens.astype(jnp.float32)
    inv_scale = lax.rsqrt(jnp.mean(widened * widened, axis=1, keepdims=True) + NORM_EPS)
    return (widened * inv_scale * norm_gain).astype(jnp.bfloat16)


def clamped_unit(gate_pre, up_pre):
    gate_clip = jnp.minimum(gate_pre, CLAMP_LIMIT)
    up_clip = jnp.clip(up_pre, -CLAMP_LIMIT, CLAMP_LIMIT)
    return ((up_clip + 1.0) * gate_clip * jax.nn.sigmoid(SLOPE_ALPHA * gate_clip)).astype(
        jnp.bfloat16
    )


def position():
    return lax.axis_index("ep").astype(jnp.int32), lax.axis_index("tp").astype(jnp.int32)


def row_split(capacity, width):
    pieces = 8 // math.gcd(capacity, 8)
    return pieces if width % (128 * pieces) == 0 else 1


def position():
    return lax.axis_index("ep").astype(jnp.int32), lax.axis_index("tp").astype(jnp.int32)


def row_split(capacity, width):
    pieces = 8 // math.gcd(capacity, 8)
    return pieces if width % (128 * pieces) == 0 else 1


def expert_column(plan):
    me, core = position()
    block = lax.broadcasted_iota(jnp.int32, (len(plan), 1), 0)
    column = jnp.zeros((len(plan), 1), jnp.int32)
    for m, (first, second) in enumerate(plan):
        column = jnp.where(block == m, jnp.where(core == 0, first, second), column)
    return jnp.bitwise_xor(column, me)


def choice_masks(routes, expert):
    return [routes[c : c + 1, :] == expert for c in range(routes.shape[0])]


def slot_ranks(routes, expert, capacity):
    tokens = routes.shape[1]
    chosen = sum(jnp.where(mask, 1.0, 0.0) for mask in choice_masks(routes, expert))
    half = tokens // 2 if capacity else tokens
    row = lax.broadcasted_iota(jnp.int32, (tokens, tokens), 0)
    column = lax.broadcasted_iota(jnp.int32, (tokens, tokens), 1)
    earlier = (row < column) & ((row >= half) == (column >= half))
    counted = jnp.dot(
        chosen.astype(jnp.bfloat16),
        jnp.where(earlier, 1.0, 0.0).astype(jnp.bfloat16),
        preferred_element_type=jnp.float32,
    )
    second = lax.broadcasted_iota(jnp.int32, (1, tokens), 1) >= half
    counted = counted + jnp.where(second, float(capacity), 0.0)
    return jnp.where(chosen > 0.0, counted, -1.0)


def block_rows(capacity, pieces):
    row = lax.broadcasted_iota(jnp.int32, (capacity * pieces, 1), 0)
    piece = sum((row >= h * capacity).astype(jnp.int32) for h in range(1, pieces)) + 0 * row
    return piece, (row - piece * capacity).astype(jnp.float32)


def load_kernel(tok_ref, gain_ref, route_ref, rate_ref, in_ref, out_ref, held_ref, norm_ref,
                gain_v, route_v, rate_v, tok_v, sems):
    _, core = position()
    pairs = ((tok_ref, tok_v), (gain_ref, gain_v), (route_ref, route_v), (rate_ref, rate_v))
    copies = [pltpu.make_async_copy(a, b, sems.at[i]) for i, (a, b) in enumerate(pairs)]
    for copy in copies:
        copy.start()
    last = sems.at[len(pairs)]

    @pl.when(core == 0)
    def _():
        pltpu.make_async_copy(in_ref, held_ref, last).start()

    @pl.when(core != 0)
    def _():
        pltpu.make_async_copy(out_ref, held_ref, last).start()

    for copy in copies:
        copy.wait()
    norm_ref[...] = rms_normed(tok_v[...], gain_v[...])
    pltpu.make_async_copy(in_ref, held_ref, last).wait()


def pack_kernel(capacity, plan, own_ref, tok2_ref, gain_ref, route_ref, route2_ref,
                norm_ref, *send_refs):
    half = own_ref.shape[0]
    rows, part = send_refs[0].shape
    pieces = rows // capacity
    norm_ref[:half, :] = own_ref[...]
    norm_ref[half:, :] = rms_normed(tok2_ref[...], gain_ref[...])
    routes = jnp.concatenate([route_ref[...], route2_ref[...]], axis=1)
    ranks = slot_ranks(routes, expert_column(plan), capacity // 2)
    piece, slot = block_rows(capacity, pieces)
    packed = None
    for h in range(pieces):
        select = jnp.concatenate(
            [
                jnp.where((ranks[m : m + 1, :] == slot) & (piece == h), 1.0, 0.0)
                for m in range(len(send_refs))
            ],
            axis=0,
        ).astype(jnp.bfloat16)
        term = jnp.dot(
            select, norm_ref[:, h * part : (h + 1) * part], preferred_element_type=jnp.float32
        )
        packed = term if packed is None else packed + term
    packed = packed.astype(jnp.bfloat16)
    for m, send_ref in enumerate(send_refs):
        send_ref[...] = packed[m * rows : (m + 1) * rows, :]


def whole_rows(block, capacity, padded):
    rows = block.shape[0]
    pieces = rows // capacity
    if pieces == 1:
        return block
    wide = block.astype(jnp.float32)
    parts = [wide[:padded]] + [
        pltpu.roll(wide, rows - h * capacity, 0)[:padded] for h in range(1, pieces)
    ]
    return jnp.concatenate(parts, axis=1).astype(jnp.bfloat16)


def split_rows(values, capacity, pieces):
    if pieces == 1:
        return values
    rows, part = capacity * pieces, values.shape[1] // pieces
    piece, _ = block_rows(capacity, pieces)
    filler = jnp.zeros((rows - values.shape[0], part), values.dtype)
    block = None
    for h in range(pieces):
        each = jnp.concatenate([values[:, h * part : (h + 1) * part], filler], axis=0)
        block = each if h == 0 else jnp.where(piece == h, pltpu.roll(each, h * capacity, 0), block)
    return block


def expert_kernel(count, capacity, halves, *refs):
    row_refs, refs = refs[:count], refs[count:]
    (gate0, up0, down0, gate1, up1, down1), out_refs = refs[:6], refs[6:]
    padded = -(-capacity // 8) * 8
    flat = jnp.concatenate([whole_rows(r[...], capacity, padded) for r in row_refs], axis=0)
    total = None
    for gate_ref, up_ref, down_ref in ((gate0, up0, down0), (gate1, up1, down1)):
        hidden = clamped_unit(
            jnp.dot(flat, gate_ref[...], preferred_element_type=jnp.float32),
            jnp.dot(flat, up_ref[...], preferred_element_type=jnp.float32),
        )
        part = jnp.dot(hidden, down_ref[...], preferred_element_type=jnp.float32)
        part = part.astype(jnp.bfloat16).astype(jnp.float32)
        total = part if total is None else total + part
    for k in range(count):
        values = total[k * padded : (k + 1) * padded, :]
        share = capacity // halves
        for j in range(halves):
            out_ref = out_refs[k * halves + j]
            part = values if j == 0 else pltpu.roll(values, padded - j * share, 0)
            part = part[: -(-share // 8) * 8]
            out_ref[...] = split_rows(part, share, out_ref.shape[0] // share).astype(jnp.bfloat16)


def weigh_kernel(capacity, pieces, plan, *refs):
    count, table_ref = (len(refs) - 1) // 2, refs[-1]
    routes = jnp.concatenate([r[...] for r in refs[:count]], axis=1)
    weights = jnp.concatenate([r[...] for r in refs[count : 2 * count]], axis=1)
    expert = expert_column(plan)
    ranks = slot_ranks(routes, expert, capacity // 2 if count == 2 else 0)
    scale = sum(
        jnp.where(mask, weights[c : c + 1, :], 0.0)
        for c, mask in enumerate(choice_masks(routes, expert))
    )
    piece, slot = block_rows(capacity, pieces)
    tokens = routes.shape[1]
    tables = [
        jnp.where(ranks[m : m + 1, :] == slot, scale[m : m + 1, :], 0.0) for m in range(len(plan))
    ]
    for h in range(pieces):
        table = jnp.concatenate([jnp.where(piece == h, t, 0.0) for t in tables], axis=0).T
        high = table.astype(jnp.bfloat16)
        low = (table - high.astype(jnp.float32)).astype(jnp.bfloat16)
        table_ref[h * tokens : (h + 1) * tokens, :] = high
        table_ref[(pieces + h) * tokens : (pieces + h + 1) * tokens, :] = low


def fetch_kernel(*refs):
    count = len(refs) // 2
    sems = refs[-1]
    copies = [
        pltpu.make_async_copy(refs[i].at[0], refs[count + i], sems.at[i]) for i in range(count)
    ]
    for copy in copies:
        copy.start()
    for copy in copies:
        copy.wait()


def join_kernel(*refs):
    at = 0
    for ref in refs[:-1]:
        refs[-1][at : at + ref.shape[0], :] = ref[...]
        at += ref.shape[0]


def shards_of(order, refs):
    place = 0
    shard = sum(r.shape[0] for r in refs) // len(order)
    for ref in refs:
        for at in range(0, ref.shape[0], shard):
            yield shard, order[place], ref, at
            place += 1


def hidden_kernel(order, norm_ref, *refs):
    held_refs, out_ref = refs[:-1], refs[-1]
    me, core = position()

    @pl.when(core == 0)
    def _():
        total = None
        for shard, offset, ref, at in shards_of(order, held_refs):
            source = pl.multiple_of(jnp.bitwise_xor(me, offset) * shard, shard)
            part = jnp.dot(
                norm_ref[:, pl.ds(source, shard)],
                ref[at : at + shard, :],
                preferred_element_type=jnp.float32,
            )
            total = part if total is None else total + part
        out_ref[...] = (total / (1.0 + jnp.exp(-total))).astype(jnp.bfloat16)

    @pl.when(core != 0)
    def _():
        out_ref[...] = jnp.zeros_like(out_ref)


def gathered(row_refs, table_ref, tokens):
    flat = jnp.concatenate([r[...] for r in row_refs], axis=0)
    part = flat.shape[1]
    sums = jnp.dot(table_ref[...], flat, preferred_element_type=jnp.float32)
    pieces = sums.shape[0] // (2 * tokens)
    for h in range(pieces):
        high = sums[h * tokens : (h + 1) * tokens]
        low = sums[(pieces + h) * tokens : (pieces + h + 1) * tokens]
        yield slice(h * part, (h + 1) * part), high + low


def early_kernel(order, held_count, table_ref, hid_ref, dgate_ref, *refs):
    held_refs, row_refs = refs[:held_count], refs[held_count:-3]
    own_ref, other_ref, sum_ref = refs[-3:]
    me, core = position()
    half = own_ref.shape[0]
    for lanes, value in gathered(row_refs, table_ref, 2 * half):
        sum_ref[:, lanes] = value

    @pl.when(core != 0)
    def _():
        hid = jnp.concatenate([hid_ref[half:, :], hid_ref[:half, :]], axis=0)
        for shard, offset, ref, at in shards_of(order, held_refs):
            lanes = pl.ds(pl.multiple_of(jnp.bitwise_xor(me, offset) * shard, shard), shard)
            branch = lax.dot_general(
                hid,
                ref[at : at + shard, :],
                (((1,), (1,)), ((), ())),
                preferred_element_type=jnp.float32,
            )
            sum_ref[:, lanes] += jax.nn.sigmoid(dgate_ref[:, lanes]) * branch

    own_ref[...] = sum_ref[:half, :]
    other_ref[...] = sum_ref[half:, :].astype(jnp.bfloat16)


def late_kernel(own_ref, share_ref, table_ref, *refs):
    row_refs, out_ref = refs[:-1], refs[-1]
    for lanes, value in gathered(row_refs, table_ref, own_ref.shape[0]):
        value = value + (own_ref[:, lanes] + share_ref[:, lanes].astype(jnp.float32))
        out_ref[:, lanes] = value.astype(jnp.bfloat16)


def call(kernel, outs, ins, scratch=(), spec=VMEM):
    if spec is HBM:
        ins = tuple(pltpu.with_memory_space_constraint(v, pltpu.HBM) for v in ins)
    return pl.pallas_call(
        kernel,
        out_shape=outs,
        in_specs=[spec for _ in ins],
        out_specs=jax.tree.map(lambda _: VMEM, outs),
        scratch_shapes=list(scratch),
        compiler_params=pltpu.CompilerParams(vmem_limit_bytes=LIMIT),
    )(*ins)


def swapped(value, offsets, cross=0):
    size = lax.axis_size("ep")
    pairs = [(2 * i + c, 2 * (i ^ offsets[c]) + (c ^ cross)) for i in range(size) for c in range(2)]
    return lax.ppermute(value, ("ep", "tp"), pairs)


def partners(value):
    return lax.ppermute(value, "tp", [(0, 1), (1, 0)])


def plan_of(sources):
    half = sources // 2
    far = [(k, k + 1) for k in range(half, sources, 2)]
    parts = (far[: len(far) // 2], [(2, 3), (0, 1)], [(k + 1, k) for k in range(4, half, 2)],
             far[len(far) // 2 :])
    plan, groups = [], []
    for part in parts:
        groups.append(list(range(len(plan), len(plan) + len(part))))
        plan += part
    return plan, groups


def bits_of(sources):
    return [1 << b for b in range(sources.bit_length() - 2, 1, -1)]


def direct_shards(
    tokens, norm_gain, routes, route_weights, w_gate, w_up, w_down, dense_in, dense_out, dense_gate
):
    tok_rows, width = tokens.shape
    sources = lax.axis_size("ep")
    own_capacity = capacity_of(tok_rows, routes.shape[1], sources)
    capacity = 2 * own_capacity
    pieces, own_pieces = row_split(capacity, width), row_split(own_capacity, width)
    bf16, f32 = jnp.bfloat16, jnp.float32
    shape = jax.ShapeDtypeStruct
    plan, (far, plane, near, last) = plan_of(sources)
    blocks = len(plan)
    direct = near + last
    homes = [offsets for m in direct for offsets in (plan[m], plan[m][::-1])]
    early = far + plane

    gain = norm_gain.reshape(1, width)
    routes, rates = routes.T, route_weights.T
    tokens2 = partners(tokens)
    routes2 = partners(routes)
    rates2 = partners(rates)
    own = (w_gate, w_up, w_down)
    other = tuple(partners(w[0]) for w in own)
    own = call(
        fetch_kernel,
        tuple(shape(w.shape[1:], w.dtype) for w in own),
        own,
        scratch=(pltpu.SemaphoreType.DMA((3,)),),
        spec=HBM,
    )

    inputs = (tokens, gain, routes, rates)
    held, norm_own, gain, routes, rates = call(
        load_kernel,
        tuple(shape(v.shape, v.dtype) for v in (dense_in,) + inputs),
        inputs + (dense_in, dense_out),
        scratch=(pltpu.VMEM(tokens.shape, bf16), pltpu.SemaphoreType.DMA((5,))),
        spec=HBM,
    )
    block = shape((capacity * pieces, width // pieces), bf16)
    normed, *sends = call(
        lambda *r: pack_kernel(capacity, plan, *r),
        (shape((2 * tok_rows, width), bf16),) + (block,) * blocks,
        (norm_own, tokens2, gain, routes, routes2),
    )
    got = [swapped(sends[m], plan[m]) for m in range(blocks)]

    order = [0]
    for bit in bits_of(sources):
        more = swapped(held, (bit, bit))
        held = call(join_kernel, shape((2 * held.shape[0], held.shape[1]), bf16), (held, more))
        order = order + [k ^ bit for k in order]
    helds = (held,) + tuple(swapped(held, (k, k)) for k in (1, 2, 3))
    order = [k ^ j for j in range(4) for k in order]

    table = call(
        lambda *r: weigh_kernel(capacity, pieces, [plan[m] for m in early], *r),
        shape((4 * tok_rows * pieces, len(early) * block.shape[0]), bf16),
        (routes, routes2, rates, rates2),
    )
    own_block = shape((own_capacity * own_pieces, width // own_pieces), bf16)
    own_table = call(
        lambda *r: weigh_kernel(own_capacity, own_pieces, homes, *r),
        shape((2 * tok_rows * own_pieces, len(homes) * own_block.shape[0]), bf16),
        (routes, rates),
    )
    dense_hidden = call(
        lambda *r: hidden_kernel(order, *r),
        shape((2 * tok_rows, dense_in.shape[1]), bf16),
        (normed,) + helds,
    )
    dense_hidden = partners(dense_hidden)
    back = {}
    for group in (plane, far, near, last):
        halves = 2 if group and group[0] in direct else 1
        outs = call(
            lambda *r, c=len(group), h=halves: expert_kernel(c, capacity, h, *r),
            (own_block if halves == 2 else block,) * (len(group) * halves),
            tuple(got[m] for m in group) + own + other,
        ) if group else ()
        for i, value in enumerate(outs):
            m, cross = group[i // halves], i % halves
            back[m, cross] = swapped(value, plan[m], cross)
    total, share = call(
        lambda *r: early_kernel(order, len(helds), *r),
        (shape((tok_rows, width), f32), shape((tok_rows, width), bf16)),
        (table, dense_hidden, dense_gate.reshape(1, width))
        + helds
        + tuple(back[m, 0] for m in early),
        scratch=(pltpu.VMEM((2 * tok_rows, width), f32),),
    )
    share = partners(share)
    return call(
        late_kernel,
        shape((tok_rows, width), bf16),
        (total, share, own_table) + tuple(back[m, c] for m in direct for c in range(2)),
    )


def rounded_term(hidden_rows, down_rows):
    partial_value = jnp.dot(hidden_rows, down_rows, preferred_element_type=jnp.float32).astype(
        jnp.bfloat16
    )
    return lax.optimization_barrier(partial_value).astype(jnp.float32)


def general_shards(
    tokens, norm_gain, routes, route_weights, w_gate, w_up, w_down, dense_in, dense_out, dense_gate
):
    tok_rows, model_width = tokens.shape
    top_count = routes.shape[1]
    sources = lax.axis_size("ep")
    experts = sources * w_gate.shape[0]
    core_count = lax.axis_size("tp")
    capacity = capacity_of(tok_rows, top_count, experts)
    entries = tok_rows * top_count
    normed = rms_normed(tokens, norm_gain)
    flat_routes = routes.reshape(entries)
    onehot = flat_routes[:, None] == lax.broadcasted_iota(jnp.int32, (1, experts), 1)
    earlier_mask = (
        lax.broadcasted_iota(jnp.int32, (entries, entries), 0)
        > lax.broadcasted_iota(jnp.int32, (entries, entries), 1)
    ).astype(jnp.bfloat16)
    counted = jnp.dot(earlier_mask, onehot.astype(jnp.bfloat16), preferred_element_type=jnp.float32)
    slot_index = jnp.sum(jnp.where(onehot, counted, 0.0), axis=1).astype(jnp.int32)
    position = flat_routes * capacity + slot_index
    places = position[None, :] == lax.broadcasted_iota(jnp.int32, (experts * capacity, 1), 0)
    filled = jnp.any(places, axis=1)
    source_entry = jnp.sum(
        jnp.where(places, lax.broadcasted_iota(jnp.int32, (1, entries), 1), 0), axis=1
    )
    buffer = jnp.where(
        filled[:, None], normed[source_entry // top_count], jnp.zeros((), jnp.bfloat16)
    )
    buffer = buffer.reshape(experts, capacity, model_width)
    gate_w, up_w, down_w = (
        lax.all_gather(w_gate[0], "tp", axis=1, tiled=True),
        lax.all_gather(w_up[0], "tp", axis=1, tiled=True),
        lax.all_gather(w_down[0], "tp", axis=0, tiled=True),
    )
    received = lax.all_to_all(buffer, "ep", split_axis=0, concat_axis=0, tiled=True)
    slot_count = received.shape[1]
    flat_rows = received.reshape(sources * slot_count, model_width)
    hidden = clamped_unit(
        jnp.dot(flat_rows, gate_w, preferred_element_type=jnp.float32),
        jnp.dot(flat_rows, up_w, preferred_element_type=jnp.float32),
    )
    half_width = hidden.shape[1] // core_count
    summed = rounded_term(hidden[:, :half_width], down_w[:half_width])
    summed = summed + rounded_term(
        hidden[:, half_width : half_width + half_width],
        down_w[half_width : half_width + half_width],
    )
    expert_out = summed.astype(jnp.bfloat16).reshape(sources, slot_count, model_width)
    returned = lax.all_to_all(expert_out, "ep", split_axis=0, concat_axis=0, tiled=True)
    flat_returned = returned.reshape(experts * capacity, model_width)
    picked = flat_returned[position].astype(jnp.float32).reshape(tok_rows, top_count, model_width)
    weighted = jnp.sum(picked * route_weights[:, :, None], axis=1)
    whole_in, whole_out = (
        lax.all_gather(dense_in, "ep", axis=0, tiled=True),
        lax.all_gather(dense_out, "ep", axis=0, tiled=True),
    )
    dense_hidden = jax.nn.silu(
        jnp.dot(normed, whole_in, preferred_element_type=jnp.float32)
    ).astype(jnp.bfloat16)
    branch = lax.dot_general(
        dense_hidden, whole_out, (((1,), (1,)), ((), ())), preferred_element_type=jnp.float32
    )
    return (weighted + jax.nn.sigmoid(dense_gate) * branch).astype(jnp.bfloat16)


def solution(mesh):
    placed = (
        P(("ep", "tp"), None),
        P(),
        P(("ep", "tp"), None),
        P(("ep", "tp"), None),
        P("ep", None, "tp"),
        P("ep", None, "tp"),
        P("ep", "tp", None),
        P("ep", None),
        P("ep", None),
        P(),
    )
    sources = mesh.shape["ep"]

    def is_direct(tokens, routes, w_gate, dense_in):
        capacity = capacity_of(tokens.shape[0] // mesh.size, routes.shape[1], sources)
        return (
            sources >= 8
            and sources & (sources - 1) == 0
            and mesh.shape["tp"] == 2
            and w_gate.shape[0] == sources
            and capacity >= 8
            and dense_in.shape[0] % (128 * sources) == 0
        )

    def mapped(shards):
        return jax.shard_map(
            shards, mesh=mesh, in_specs=placed, out_specs=P(("ep", "tp"), None), check_vma=False
        )

    def step(*arrays):
        tokens, routes, w_gate, dense_in = arrays[0], arrays[2], arrays[4], arrays[7]
        if is_direct(tokens, routes, w_gate, dense_in):
            return mapped(direct_shards)(*arrays)
        return mapped(general_shards)(*arrays)

    return step
```
